128 devices in a mesh: sp: 16 (over z, x), tp: 8 (over y, core).
Axes of the slice: x: 4, y: 4, z: 4, core: 2. Of those that a mesh axis runs over, the one named last changes fastest.
Arguments:
- resid: bfloat16 [12288, 2048], P(('sp', 'tp')), may hold values from -6 to 6
- queries: bfloat16 [12288, 1024], P('sp', 'tp'), may hold values from -160 to 160
- keys: bfloat16 [12288, 1024], P('sp', 'tp'), may hold values from -6 to 6
- values: bfloat16 [12288, 1024], P('sp', 'tp'), may hold values from -6 to 6
- cum_gate: float32 [12288, 16], P('sp', 'tp'), may hold values from -1385 to 0, as said below
- out_weight: bfloat16 [1024, 2048], P('tp'), may hold values from -0.375 to 0.375
- norm_gain: float32 [2048], replicated, may hold values from 0.1 to 1.9
- gate_weight: bfloat16 [2048, 5504], P('sp', 'tp'), may hold values from -0.125 to 0.125
- up_weight: bfloat16 [2048, 5504], P('sp', 'tp'), may hold values from -0.125 to 0.125
- down_weight: bfloat16 [5504, 2048], P('tp', 'sp'), may hold values from -0.078125 to 0.078125
Outputs:
- layer_out: bfloat16 [12288, 2048], P(('sp', 'tp'))
The draws below stay inside these ranges and needn't reach their ends.
Inputs may be any that keep to these rules, and one draw needn't show every extreme that they name: `cum_gate`: each column is non-increasing along positions and starts at or below zero.
All inputs are finite; a program needn't handle non-finite values.
Results may differ from the reference program's by a relative error of at most 0.01.
Values may be sent and summed in bfloat16 or wider, within the bound.
A program may use at most 256 MiB of HBM per device.

```python
import jax
import jax.numpy as jnp
from jax import lax

D = 2048
HEAD_COUNT = 16
HEAD_DIM = 64
FF = 5504
TOK_DEV = 768
TOKEN_COUNT = 12288
N_SP = 16
N_TP = 8


def paired_rows(key):
    key_query, key_key = jax.random.split(jax.random.fold_in(key, 11))
    width = HEAD_COUNT * HEAD_DIM
    queries = 2.5 * jnp.clip(jax.random.normal(key_query, (TOKEN_COUNT, width), jnp.float32), -5.0, 5.0)
    keys = jnp.clip(jax.random.normal(key_key, (TOKEN_COUNT, width), jnp.float32), -5.0, 5.0)
    return (queries, keys)


def draw_queries(key, part):
    return paired_rows(key)[0].astype(jnp.bfloat16)


def draw_keys(key, part):
    return paired_rows(key)[1].astype(jnp.bfloat16)


def draw_cum_gate(key, part):
    key_fast, key_block, key_rough, key_index_offset, key_length = jax.random.split(jax.random.fold_in(key, 23), 5)
    fast = jax.random.randint(key_fast, (HEAD_COUNT,), 0, 2).astype(jnp.float32)
    blocks = TOKEN_COUNT // TOK_DEV
    block_factor = jnp.exp(jax.random.uniform(key_block, (blocks, 1), jnp.float32, 0.0, jnp.log(3.0)))
    block_factor = jnp.repeat(block_factor, TOK_DEV, axis=0)
    rough = jax.random.uniform(key_rough, (TOKEN_COUNT, HEAD_COUNT), jnp.float32, 0.5, 1.5)
    base = fast * (1.0 / 40.0) + (1.0 - fast) * (0.6 / TOKEN_COUNT)
    stride_offset = -base[None, :] * block_factor * rough
    group_row_block = jax.random.randint(key_index_offset, (4,), 0, TOKEN_COUNT)
    group_row_count = jnp.log(jax.random.uniform(key_length, (4, HEAD_COUNT), jnp.float32, 0.5, 0.8))
    stride_offset = stride_offset.at[group_row_block].add(group_row_count)
    return jnp.cumsum(stride_offset, axis=0)


def block_scale(key, dims, shards, least, largest):
    def one(dim, parts):
        draws = jax.random.uniform(jax.random.fold_in(jax.random.fold_in(key, 6), dim), (parts,), jnp.float32, least / len(shards), largest / len(shards))
        return jnp.repeat(jnp.exp(draws), dims[dim] // parts).reshape((-1,) + (1,) * (len(dims) - dim - 1))

    factor_of = one(*shards[0])
    for cut in shards[1:]:
        factor_of = factor_of * one(*cut)
    return factor_of


def normal_values(rng, dims, spread, limit, pieces=(), held_as=jnp.bfloat16):
    entries = jax.random.normal(rng, dims, jnp.float32) * spread
    if len(pieces) > 0:
        entries = block_scale(rng, dims, pieces, -0.22, 0.18) * entries
    return jnp.clip(entries, min=-limit, max=limit).astype(held_as)


def setup_inputs(seed: int = 0) -> dict:
    key_of = jax.random.split(jax.random.key(seed), 11)
    resid = normal_values(key_of[0], (TOKEN_COUNT, D), 1.0, 6.0, ((0, 128),))
    queries = draw_queries(jax.random.fold_in(key_of[10], 71), 0)
    keys = draw_keys(jax.random.fold_in(key_of[10], 71), 0)
    values = normal_values(key_of[3], (TOKEN_COUNT, HEAD_COUNT * HEAD_DIM), 1.0, 6.0, ((0, 16), (1, 8)))
    cum_gate = draw_cum_gate(jax.random.fold_in(key_of[10], 71), 0)
    out_weight = normal_values(key_of[5], (HEAD_COUNT * HEAD_DIM, D), (HEAD_COUNT * HEAD_DIM // 4) ** -0.5, 0.375, ((0, 8),))
    norm_gain = jnp.clip(1.0 + 0.18 * jax.random.normal(key_of[6], (D,), jnp.float32), 0.1, 1.9)
    gate_weight = normal_values(key_of[7], (D, FF), D ** -0.5, 0.125, ((0, 16), (1, 8)))
    up_weight = normal_values(key_of[8], (D, FF), D ** -0.5, 0.125, ((0, 16), (1, 8)))
    down_weight = normal_values(key_of[9], (FF, D), FF ** -0.5, 0.078125, ((0, 8), (1, 16)))
    return dict(resid=resid, queries=queries, keys=keys, values=values, cum_gate=cum_gate, out_weight=out_weight, norm_gain=norm_gain, gate_weight=gate_weight, up_weight=up_weight, down_weight=down_weight)


def reference(resid, queries, keys, values, cum_gate, out_weight, norm_gain, gate_weight, up_weight, down_weight):
    width = HEAD_COUNT * HEAD_DIM
    total_len = queries.shape[0]
    scale = HEAD_DIM ** (-0.5)
    key_heads = keys.astype(jnp.float32).reshape(total_len, HEAD_COUNT, HEAD_DIM).transpose(1, 0, 2)
    value_heads = values.astype(jnp.float32).reshape(total_len, HEAD_COUNT, HEAD_DIM).transpose(1, 0, 2)
    key_pos = jnp.arange(total_len, dtype=jnp.int32)
    gate_rows = cum_gate.T

    def block(index):
        start = (index * TOK_DEV).astype(jnp.int32)
        query_block = lax.dynamic_slice_in_dim(queries, start, TOK_DEV, 0).astype(jnp.float32)
        query_block = query_block.reshape(TOK_DEV, HEAD_COUNT, HEAD_DIM).transpose(1, 0, 2)
        gate_block = lax.dynamic_slice_in_dim(cum_gate, start, TOK_DEV, 0).T
        score = jnp.einsum('hqd,hkd->hqk', query_block, key_heads) * scale
        score = score + gate_block[:, :, None] - gate_rows[:, None, :]
        query_pos = start + jnp.arange(TOK_DEV, dtype=jnp.int32)
        score = jnp.where(key_pos[None, None, :] <= query_pos[None, :, None], score, -jnp.inf)
        top = lax.optimization_barrier(jnp.max(score, axis=-1, keepdims=True))
        weight = jnp.exp(score - top)
        total = lax.optimization_barrier(jnp.sum(weight, axis=-1, keepdims=True))
        weight_b = lax.optimization_barrier(weight.astype(jnp.bfloat16)).astype(jnp.float32)
        numer = jnp.einsum('hqk,hkd->hqd', weight_b, value_heads)
        result = (numer / total).transpose(1, 0, 2).reshape(TOK_DEV, width)
        return result.astype(jnp.bfloat16)
    attn = lax.map(block, jnp.arange(N_SP, dtype=jnp.int32)).reshape(total_len, width)
    group = width // N_TP
    proj = jnp.zeros((total_len, D), jnp.float32)
    for index in range(N_TP):
        term = jnp.dot(attn[:, index * group:(index + 1) * group], out_weight[index * group:(index + 1) * group], preferred_element_type=jnp.float32)
        proj = proj + lax.optimization_barrier(term.astype(jnp.bfloat16)).astype(jnp.float32)
    mixed = resid.astype(jnp.float32) + proj
    normed = (mixed * lax.rsqrt(lax.optimization_barrier(jnp.mean(mixed * mixed, axis=-1, keepdims=True)) + 1e-06) * norm_gain).astype(jnp.bfloat16)
    gate = jnp.dot(normed, gate_weight, preferred_element_type=jnp.float32)
    upper = jnp.dot(normed, up_weight, preferred_element_type=jnp.float32)
    hidden = (jax.nn.silu(gate) * upper).astype(jnp.bfloat16)
    hid_group = FF // N_TP
    ffn = jnp.zeros((total_len, D), jnp.float32)
    for index in range(N_TP):
        term = jnp.dot(hidden[:, index * hid_group:(index + 1) * hid_group], down_weight[index * hid_group:(index + 1) * hid_group], preferred_element_type=jnp.float32)
        ffn = ffn + lax.optimization_barrier(term.astype(jnp.bfloat16)).astype(jnp.float32)
    return (mixed + 0.5 * ffn).astype(jnp.bfloat16)
```

```python
import functools

import jax
import jax.numpy as jnp
from jax import lax
from jax.experimental import pallas as pl
from jax.experimental.pallas import tpu as pltpu
from jax.sharding import PartitionSpec as P

HEAD_DIM = 64
ROWS = 768
OWN = 96
D = 2048
FFW = 688
GUW = 1408
N_SP = 16
LOOK = 3
BF = jnp.bfloat16
F32 = jnp.float32
MESH = pl.DeviceIdType.MESH
NT = (((1,), (1,)), ((), ()))

N_PIECE = 7
SIGN = (1, 1, -1, 1, -1, 1, -1)


def gray(n):
    return n + (n // 2) * (1 - 2 * (n % 2))


def kernel(
    q_ref, k_ref, v_ref, g_ref, ow_ref, wgu_ref, wd_ref, resid_ref, gain_ref,
    out_ref,
    GG, GK, GV, GW, GD, GO, QZ, ACC, MX, ATL, AT, MIX, NA, HID, SB, RB, PA, TB, RR,
    rs, ss, ors, oss, nrs, nss, ars, ass, brs, bss, crs, css, lsem,
):
    sp = lax.axis_index("sp")
    tp = lax.axis_index("tp")
    c = tp % 2
    y = tp // 2
    z = sp // 4
    x = sp % 4
    a = z + c * (x - z)
    b = x + c * (z - x)

    def spof(da, db):
        return ((a + da + 4) % 4) * (4 - 3 * c) + ((b + db + 4) % 4) * (1 + 3 * c)

    def tpof(yy, cc):
        return yy * 2 + cc

    sib = tpof(y, 1 - c)

    bar = pltpu.get_barrier_semaphore()
    for da, db in ((1, 0), (3, 0), (0, 1), (0, 3)):
        pl.semaphore_signal(bar, inc=1, device_id=(spof(da, db), tp), device_id_type=MESH)
    for i in range(1, 8):
        pl.semaphore_signal(bar, inc=1, device_id=(sp, (tp + i) % 8), device_id_type=MESH)

    def part(p, s):
        if p == 0:
            return GG.at[s]
        if p == 1:
            return GK.at[pl.ds(pl.multiple_of(s * ROWS, ROWS), ROWS)]
        if p == 2:
            return GV.at[pl.ds(pl.multiple_of(s * ROWS, ROWS), ROWS)]
        if p == 3:
            return GW.at[pl.ds(pl.multiple_of(s * 128, 64), 64)]
        if p == 4:
            return GW.at[pl.ds(pl.multiple_of(s * 128 + 64, 64), 64)]
        if p == 5:
            return GD.at[pl.ds(0, 352), pl.ds(pl.multiple_of(s * 128, 128), 128)]
        return GD.at[pl.ds(352, 336), pl.ds(pl.multiple_of(s * 128, 128), 128)]

    local = [
        pltpu.make_async_copy(g_ref, part(0, sp), lsem.at[0]),
        pltpu.make_async_copy(k_ref, part(1, sp), lsem.at[1]),
        pltpu.make_async_copy(v_ref, part(2, sp), lsem.at[2]),
        pltpu.make_async_copy(wgu_ref, GW.at[pl.ds(pl.multiple_of(sp * 128, 128), 128)], lsem.at[3]),
        pltpu.make_async_copy(wd_ref, GD.at[:, pl.ds(pl.multiple_of(sp * 128, 128), 128)], lsem.at[4]),
        pltpu.make_async_copy(ow_ref, GO.at[pl.ds(pl.multiple_of(tp * 128, 128), 128)], lsem.at[5]),
    ]
    for cp in local:
        cp.start()

    def copy(p, s, idx, dst):
        return pltpu.make_async_remote_copy(
            src_ref=part(p, s), dst_ref=part(p, s), send_sem=ss.at[p, idx], recv_sem=rs.at[p, s],
            device_id=(dst, tp), device_id_type=MESH,
        )

    def begin(p):
        copy(p, sp, 2, spof(0, 1)).start()
        copy(p, sp, 3, spof(0, 3)).start()
        copy(p, sp, 0, spof(1, 0)).start()
        copy(p, sp, 1, spof(3, 0)).start()

    def serve(p, k):
        da = gray(k % 4)
        db = gray(k // 4)
        s = spof(da, db)
        copy(p, s, 0, sp).wait_recv()
        d = SIGN[p]
        back = (4 - d) % 4

        @pl.when((k < 4) & (da == back))
        def _():
            copy(p, s, 10, spof(d, 0)).start()

        @pl.when(k < 4)
        def _():
            copy(p, s, 2 + 2 * k, spof(0, 1)).start()
            copy(p, s, 3 + 2 * k, spof(0, 3)).start()

        @pl.when(db == back)
        def _():
            copy(p, s, 11 + k % 4, spof(0, d)).start()

    def serve_own(p):
        pass

    dy = 1 - 2 * c

    def yat(n):
        return (y + n + 4) % 4

    def ycopy(block, sems, rsems, idx, slot, dst):
        return pltpu.make_async_remote_copy(
            src_ref=block(slot), dst_ref=block(slot), send_sem=sems.at[idx], recv_sem=rsems.at[slot],
            device_id=(sp, dst), device_id_type=MESH,
        )

    def slot_of(yy, cc):
        return cc * 4 + yy

    def ybegin(block, sems, rsems):
        own = slot_of(y, c)
        ycopy(block, sems, rsems, 0, own, tpof(yat(dy), c)).start()
        ycopy(block, sems, rsems, 1, own, tpof(yat(-dy), c)).start()
        ycopy(block, sems, rsems, 2, own, sib).start()

    def yserve(block, sems, rsems, n):
        if n == 0:
            s = slot_of(yat(-dy), c)
            ycopy(block, sems, rsems, 0, s, sib).wait_recv()
            ycopy(block, sems, rsems, 3, s, tpof(yat(dy), c)).start()
            ycopy(block, sems, rsems, 4, s, sib).start()
        elif n == 1:
            s = slot_of(yat(dy), c)
            ycopy(block, sems, rsems, 0, s, sib).wait_recv()
            ycopy(block, sems, rsems, 5, s, sib).start()
        else:
            s = slot_of(yat(2), c)
            ycopy(block, sems, rsems, 0, s, sib).wait_recv()
            ycopy(block, sems, rsems, 6, s, sib).start()

    def yfinish(block, sems, rsems):
        for n in range(4):
            s = slot_of(yat(n), 1 - c)
            ycopy(block, sems, rsems, 0, s, sib).wait_recv()

    def oblock(slot):
        t = (slot % 4) * 2 + slot // 4
        return GO.at[pl.ds(pl.multiple_of(t * 128, 128), 128)]

    def nblock(slot):
        return NA.at[pl.ds(pl.multiple_of(slot * OWN, OWN), OWN)]

    lane = lax.broadcasted_iota(jnp.int32, (ROWS, 128), 1)
    qs = q_ref[...].astype(F32) * (HEAD_DIM ** (-0.5))
    QZ[0] = jnp.where(lane < HEAD_DIM, qs, 0.0).astype(BF)
    QZ[1] = jnp.where(lane >= HEAD_DIM, qs, 0.0).astype(BF)

    for cp in local:
        cp.wait()
    pl.semaphore_wait(bar, 11)
    for p in (1, 2, 0):
        begin(p)
    ybegin(oblock, oss, ors)

    def scores(h, r0, n, s, width):
        qh = QZ[h, pl.ds(r0, n), :]
        kb = GK[pl.ds(pl.multiple_of(s * ROWS, ROWS), width), :]
        sc = lax.dot_general(qh, kb, NT, preferred_element_type=F32)
        return sc - GG[s, h : h + 1, :width]

    def values_of(s, width):
        vb = GV[pl.ds(pl.multiple_of(s * ROWS, ROWS), width), :]
        return jnp.concatenate([vb, jnp.ones((width, 128), BF)], axis=1)

    QB = 256
    for i in range(ROWS // QB):
        width = QB * (i + 1)
        row = lax.broadcasted_iota(jnp.int32, (QB, width), 0) + i * QB
        col = lax.broadcasted_iota(jnp.int32, (QB, width), 1)
        for h in range(2):
            sc = jnp.where(col <= row, scores(h, i * QB, QB, sp, width), -1e30)
            top = jnp.broadcast_to(jnp.max(sc, axis=1, keepdims=True), (QB, 128))
            wt = jnp.exp(sc - jnp.concatenate([top] * (width // 128), axis=1))
            ACC[h, i * QB : (i + 1) * QB, :] = jnp.dot(
                wt.astype(BF), values_of(sp, width), preferred_element_type=F32
            )
            MX[h, i * QB : (i + 1) * QB, :] = top

    def tile(s):
        def chunk(i, _):
            r0 = pl.multiple_of(i * QB, QB)
            for h in range(2):
                sc = scores(h, r0, QB, s, ROWS)
                old = MX[h, pl.ds(r0, QB), :]
                top = jnp.maximum(old, jnp.max(sc, axis=1, keepdims=True))
                wt = jnp.exp(sc - jnp.concatenate([top] * (ROWS // 128), axis=1))
                fade = jnp.exp(old - top)
                pv = jnp.dot(wt.astype(BF), values_of(s, ROWS), preferred_element_type=F32)
                ACC[h, pl.ds(r0, QB), :] = (
                    ACC[h, pl.ds(r0, QB), :] * jnp.concatenate([fade, fade], axis=1) + pv
                )
                MX[h, pl.ds(r0, QB), :] = top
            return 0

        lax.fori_loop(0, ROWS // QB, chunk, 0)

    KV = (1, 2, 0)
    for k in range(1, LOOK + 1):
        for p in KV:
            serve(p, k)

    def step(k, _):
        @pl.when(k + LOOK < N_SP)
        def _():
            for p in KV:
                serve(p, k + LOOK)

        @pl.when(k == 3)
        def _():
            yserve(oblock, oss, ors, 0)
            yserve(oblock, oss, ors, 1)

        @pl.when(k == 8)
        def _():
            yserve(oblock, oss, ors, 2)
            begin(3)
            begin(4)

        @pl.when(k == 12)
        def _():
            for p in (3, 4):
                for kk in range(1, 4):
                    serve(p, kk)
            begin(5)
            begin(6)

        s = spof(gray(k % 4), gray(k // 4))

        @pl.when(s < sp)
        def _():
            tile(s)

        return 0

    lax.fori_loop(1, N_SP, step, 0)

    first = lax.broadcasted_iota(jnp.int32, (ROWS, 128), 1) < HEAD_DIM
    o0 = ACC[0, :, :128] / ACC[0, :, 128:]
    o1 = ACC[1, :, :128] / ACC[1, :, 128:]
    ATL[...] = jnp.where(first, o0, o1).astype(BF)

    def acopy(i, src, dst, slot):
        return pltpu.make_async_remote_copy(
            src_ref=ATL.at[pl.ds(pl.multiple_of(dst * OWN, 32), OWN)],
            dst_ref=AT.at[:, pl.ds(pl.multiple_of(slot * 128, 128), 128)],
            send_sem=ass.at[i], recv_sem=ars.at[slot], device_id=(sp, dst), device_id_type=MESH,
        )

    for i in range(1, 8):
        acopy(i - 1, tp, (tp + i) % 8, tp).start()
    AT[:, pl.ds(pl.multiple_of(tp * 128, 128), 128)] = ATL[pl.ds(pl.multiple_of(tp * OWN, 32), OWN), :]
    yfinish(oblock, oss, ors)
    for p in (3, 4):
        for kk in range(4, 8):
            serve(p, kk)
    for i in range(1, 8):
        t = (tp + i) % 8
        acopy(0, tp, t, t).wait_recv()

    NB = 512
    sq = jnp.zeros((OWN, 1), F32)
    for j in range(D // NB):
        pj = jnp.dot(AT[...], GO[:, j * NB : (j + 1) * NB], preferred_element_type=F32)
        mj = resid_ref[:, j * NB : (j + 1) * NB].astype(F32) + pj
        MIX[:, j * NB : (j + 1) * NB] = mj
        sq = sq + jnp.sum(mj * mj, axis=1, keepdims=True)
    inv = lax.rsqrt(sq * (1.0 / D) + 1e-6)
    own_slot = slot_of(y, c)
    NA[pl.ds(pl.multiple_of(own_slot * OWN, OWN), OWN), :] = (MIX[...] * inv * gain_ref[...]).astype(BF)
    ybegin(nblock, nss, nrs)
    for p in (5, 6):
        for kk in range(1, 4):
            serve(p, kk)
    for p in (3, 4):
        for kk in range(8, 12):
            serve(p, kk)
    yserve(nblock, nss, nrs, 0)
    yserve(nblock, nss, nrs, 1)
    yserve(nblock, nss, nrs, 2)
    for p in (5, 6):
        for kk in range(4, 12):
            serve(p, kk)
    yfinish(nblock, nss, nrs)
    for p in (3, 4):
        for kk in range(12, 16):
            serve(p, kk)

    def gu(j, _):
        col = pl.multiple_of(j * 256, 256)
        r = jnp.dot(NA[...], GW[:, pl.ds(col, 256)], preferred_element_type=F32)
        gt = r[:, :128]
        HID[:, pl.ds(pl.multiple_of(j * 128, 128), 128)] = (gt / (1.0 + jnp.exp(-gt)) * r[:, 128:]).astype(BF)
        return 0

    lax.fori_loop(0, 5, gu, 0)
    r = jnp.dot(NA[...], GW[:, 1280:1408], preferred_element_type=F32)
    gt = r[:, :48]
    HID[:, 640:688] = (gt / (1.0 + jnp.exp(-gt)) * r[:, 48:96]).astype(BF)
    for p in (5, 6):
        for kk in range(12, 16):
            serve(p, kk)

    half = 4 * OWN

    def scopy(n):
        blk = yat(2 + n)
        view = pl.ds(pl.multiple_of(blk * OWN, OWN), OWN)
        return pltpu.make_async_remote_copy(
            src_ref=SB.at[view], dst_ref=RB.at[view], send_sem=bss.at[blk], recv_sem=brs.at[blk],
            device_id=(sp, sib), device_id_type=MESH,
        )

    hs = HID[pl.ds(pl.multiple_of((1 - c) * half, half), half), :]
    for j in range(D // NB):
        SB[:, j * NB : (j + 1) * NB] = jnp.dot(
            hs, GD[:, j * NB : (j + 1) * NB], preferred_element_type=F32
        ).astype(BF)
    for n in range(4):
        scopy(n).start()
    ho = HID[pl.ds(pl.multiple_of(c * half, half), half), :]
    for j in range(D // NB):
        PA[:, j * NB : (j + 1) * NB] = jnp.dot(ho, GD[:, j * NB : (j + 1) * NB], preferred_element_type=F32)
    for n in range(4):
        scopy(n).wait_recv()

    def both(n):
        view = pl.ds(pl.multiple_of(yat(n) * OWN, OWN), OWN)
        return PA[view, :] + RB[view, :].astype(F32)

    def rcopy(n, to):
        return pltpu.make_async_remote_copy(
            src_ref=TB.at[n], dst_ref=RR.at[n], send_sem=css.at[n], recv_sem=crs.at[n],
            device_id=(sp, tpof(yat(to), c)), device_id_type=MESH,
        )

    TB[0] = both(2).astype(BF)
    rcopy(0, dy).start()
    TB[1] = both(-dy).astype(BF)
    rcopy(1, -dy).start()
    rcopy(0, dy).wait_recv()
    TB[2] = (both(dy) + RR[0].astype(F32)).astype(BF)
    rcopy(2, dy).start()
    rcopy(1, -dy).wait_recv()
    rcopy(2, dy).wait_recv()
    ffn = both(0) + RR[1].astype(F32) + RR[2].astype(F32)
    out_ref[...] = (MIX[...] + 0.5 * ffn).astype(BF)

    for n in range(3):
        rcopy(n, dy).wait_send()
    for n in range(4):
        scopy(n).wait_send()
    for i in range(1, 8):
        acopy(i - 1, tp, (tp + i) % 8, tp).wait_send()
    for i in range(7):
        ycopy(oblock, oss, ors, i, slot_of(y, c), sib).wait_send()
        ycopy(nblock, nss, nrs, i, slot_of(y, c), sib).wait_send()
    for p in range(N_PIECE):

        def drain(i, _):
            copy(p, sp, i, sp).wait_send()
            return 0

        lax.fori_loop(0, 15, drain, 0)


def local(resid, queries, keys, values, cum_gate, out_weight, norm_gain, gate_weight, up_weight, down_weight):
    gates = jnp.pad(cum_gate.T, ((0, 6), (0, 0)))
    cols = []
    for j in range(5):
        cols += [gate_weight[:, j * 128 : (j + 1) * 128], up_weight[:, j * 128 : (j + 1) * 128]]
    cols += [gate_weight[:, 640:], up_weight[:, 640:], jnp.zeros((128, 32), BF)]
    gate_up = jnp.concatenate(cols, axis=1)
    vm = pl.BlockSpec(memory_space=pltpu.VMEM)
    hbm = pl.BlockSpec(memory_space=pl.ANY)
    dma = pltpu.SemaphoreType.DMA
    V = pltpu.VMEM
    return pl.pallas_call(
        kernel,
        out_shape=jax.ShapeDtypeStruct((OWN, D), BF),
        in_specs=[vm, hbm, hbm, hbm, hbm, hbm, hbm, vm, vm],
        out_specs=vm,
        scratch_shapes=[
            V((N_SP, 8, ROWS), F32),
            V((N_SP * ROWS, 128), BF),
            V((N_SP * ROWS, 128), BF),
            V((D, GUW), BF),
            V((FFW, D), BF),
            V((1024, D), BF),
            V((2, ROWS, 128), BF),
            V((2, ROWS, 256), F32),
            V((2, ROWS, 128), F32),
            V((ROWS, 128), BF),
            V((OWN, 1024), BF),
            V((OWN, D), F32),
            V((ROWS, D), BF),
            V((ROWS, FFW), BF),
            V((4 * OWN, D), BF),
            V((4 * OWN, D), BF),
            V((4 * OWN, D), F32),
            V((3, OWN, D), BF),
            V((3, OWN, D), BF),
            dma((N_PIECE, N_SP)),
            dma((N_PIECE, 15)),
            dma((8,)),
            dma((7,)),
            dma((8,)),
            dma((7,)),
            dma((8,)),
            dma((7,)),
            dma((4,)),
            dma((4,)),
            dma((3,)),
            dma((3,)),
            dma((6,)),
        ],
        compiler_params=pltpu.CompilerParams(
            collective_id=0, has_side_effects=True, vmem_limit_bytes=64 * 1024 * 1024 - 128 * 1024
        ),
        name="layer",
    )(queries, keys, values, gates, out_weight, gate_up, down_weight, resid, norm_gain.reshape(1, D))


def solution(mesh):
    return jax.shard_map(
        local,
        mesh=mesh,
        in_specs=(
            P(("sp", "tp"), None),
            P("sp", "tp"),
            P("sp", "tp"),
            P("sp", "tp"),
            P("sp", "tp"),
            P("tp", None),
            P(),
            P("sp", "tp"),
            P("sp", "tp"),
            P("tp", "sp"),
        ),
        out_specs=P(("sp", "tp"), None),
        check_vma=False,
    )
```

```python
import functools

import jax
import jax.numpy as jnp
from jax import lax
from jax.experimental import pallas as pl
from jax.experimental.pallas import tpu as pltpu
from jax.sharding import PartitionSpec as P

HEAD_DIM = 64
ROWS = 768
OWN = 96
D = 2048
FFW = 688
GUW = 1408
N_SP = 16
HQ = ROWS // 2
KV = (1, 2, 0)
LOOK = 1
K_O1 = 6
K_O2 = 10
K_W = 5
K_WS = 12
WEIGHTS = (3, 4, 5, 6)
BF = jnp.bfloat16
F32 = jnp.float32
MESH = pl.DeviceIdType.MESH
NT = (((1,), (1,)), ((), ()))

N_PIECE = 7
SIGN = (1, 1, -1, 1, -1, 1, -1)


WAVE = (
    (0, 0), (1, 0), (3, 0), (0, 1), (0, 3), (2, 0), (1, 1), (3, 1),
    (1, 3), (3, 3), (0, 2), (2, 1), (2, 3), (1, 2), (3, 2), (2, 2),
)


def offsets(k):
    if isinstance(k, int):
        return WAVE[k]
    da, db = jnp.int32(0), jnp.int32(0)
    for n in range(1, 16):
        da = jnp.where(k == n, WAVE[n][0], da)
        db = jnp.where(k == n, WAVE[n][1], db)
    return da, db


def kernel(
    q_ref, k_ref, v_ref, g_ref, ow_ref, wg_in, wu_in, wd_ref, resid_in, gain_in,
    out_hbm,
    GG, GK, GV, GW, GD, GO, QR, QZ, ACC, MX, ATL, AT, MIX, NA, HID, SB, RB, PA, TB, RR,
    wg_ref, wu_ref, resid_ref, gain_ref, out_ref,
    rs, ss, ors, oss, nrs, nss, ars, ass, brs, bss, crs, css, lsem, qsem, osem,
):
    sp = lax.axis_index("sp")
    tp = lax.axis_index("tp")
    c = tp % 2
    y = tp // 2
    z = sp // 4
    x = sp % 4
    a = z + c * (x - z)
    b = x + c * (z - x)

    def spof(da, db):
        return ((a + da + 4) % 4) * (4 - 3 * c) + ((b + db + 4) % 4) * (1 + 3 * c)

    def tpof(yy, cc):
        return yy * 2 + cc

    sib = tpof(y, 1 - c)
    ps = N_SP - 1 - sp

    bar = pltpu.get_barrier_semaphore()
    for da, db in ((1, 0), (3, 0), (0, 1), (0, 3)):
        pl.semaphore_signal(bar, inc=1, device_id=(spof(da, db), tp), device_id_type=MESH)
    for i in range(8):
        if i:
            pl.semaphore_signal(bar, inc=1, device_id=(sp, (tp + i) % 8), device_id_type=MESH)
        pl.semaphore_signal(bar, inc=1, device_id=(ps, (tp + i) % 8), device_id_type=MESH)

    def part(p, s):
        if p == 0:
            return GG.at[s]
        if p == 1:
            return GK.at[pl.ds(pl.multiple_of(s * ROWS, ROWS), ROWS)]
        if p == 2:
            return GV.at[pl.ds(pl.multiple_of(s * ROWS, ROWS), ROWS)]
        if p == 3:
            return GW.at[pl.ds(pl.multiple_of(s * 128, 64), 64)]
        if p == 4:
            return GW.at[pl.ds(pl.multiple_of(s * 128 + 64, 64), 64)]
        if p == 5:
            return GD.at[pl.ds(0, 352), pl.ds(pl.multiple_of(s * 128, 128), 128)]
        return GD.at[pl.ds(352, 336), pl.ds(pl.multiple_of(s * 128, 128), 128)]

    local = [
        pltpu.make_async_copy(g_ref, part(0, sp), lsem.at[0]),
        pltpu.make_async_copy(k_ref, part(1, sp), lsem.at[1]),
        pltpu.make_async_copy(v_ref, part(2, sp), lsem.at[2]),
        pltpu.make_async_copy(wd_ref, GD.at[:, pl.ds(pl.multiple_of(sp * 128, 128), 128)], lsem.at[3]),
        pltpu.make_async_copy(ow_ref, GO.at[pl.ds(pl.multiple_of(tp * 128, 128), 128)], lsem.at[4]),
        pltpu.make_async_copy(wg_in, wg_ref, lsem.at[5]),
        pltpu.make_async_copy(wu_in, wu_ref, lsem.at[6]),
        pltpu.make_async_copy(resid_in, resid_ref, lsem.at[7]),
        pltpu.make_async_copy(gain_in, gain_ref, lsem.at[8]),
    ]
    for cp in local:
        cp.start()

    def copy(p, s, idx, dst):
        return pltpu.make_async_remote_copy(
            src_ref=part(p, s), dst_ref=part(p, s), send_sem=ss.at[p, idx], recv_sem=rs.at[p, s],
            device_id=(dst, tp), device_id_type=MESH,
        )

    def begin_first(p):
        copy(p, sp, 0, spof(1, 0)).start()
        copy(p, sp, 1, spof(3, 0)).start()

    def send_second(p, da):
        s = spof(da, 0)
        copy(p, s, 2 + 2 * da, spof(0, 1)).start()
        copy(p, s, 3 + 2 * da, spof(0, 3)).start()

    def begin(p):
        begin_first(p)
        send_second(p, 0)

    def serve_first(p, da):
        s = spof(da, 0)
        copy(p, s, 0, sp).wait_recv()
        d = SIGN[p]
        if da == (4 - d) % 4:
            copy(p, s, 10, spof(d, 0)).start()

    def relay(p):
        d = SIGN[p]
        for da in (0, 1, 3, 2):
            s = spof(da, 4 - d)
            copy(p, s, 0, sp).wait_recv()
            copy(p, s, 11 + da, spof(0, d)).start()

    def collect(p):
        d = SIGN[p]
        for db in (4 + d, 2):
            for da in (0, 1, 3, 2):
                copy(p, spof(da, db), 0, sp).wait_recv()

    def serve(p, k):
        da, db = offsets(k)
        s = spof(da, db)
        copy(p, s, 0, sp).wait_recv()
        d = SIGN[p]
        back = (4 - d) % 4

        @pl.when((db == 0) & (da == back))
        def _():
            copy(p, s, 10, spof(d, 0)).start()

        @pl.when(db == 0)
        def _():
            copy(p, s, 2 + 2 * da, spof(0, 1)).start()
            copy(p, s, 3 + 2 * da, spof(0, 3)).start()

        @pl.when(db == back)
        def _():
            copy(p, s, 11 + da, spof(0, d)).start()

    dy = 1 - 2 * c

    def yat(n):
        return (y + n + 4) % 4

    def ycopy(block, sems, rsems, idx, slot, dst):
        return pltpu.make_async_remote_copy(
            src_ref=block(slot), dst_ref=block(slot), send_sem=sems.at[idx], recv_sem=rsems.at[slot],
            device_id=(sp, dst), device_id_type=MESH,
        )

    def slot_of(yy, cc):
        return cc * 4 + yy

    def ybegin(block, sems, rsems):
        own = slot_of(y, c)
        ycopy(block, sems, rsems, 0, own, tpof(yat(dy), c)).start()
        ycopy(block, sems, rsems, 1, own, tpof(yat(-dy), c)).start()
        ycopy(block, sems, rsems, 2, own, sib).start()

    def yserve(block, sems, rsems, n):
        if n == 0:
            s = slot_of(yat(-dy), c)
            ycopy(block, sems, rsems, 0, s, sib).wait_recv()
            ycopy(block, sems, rsems, 3, s, tpof(yat(dy), c)).start()
            ycopy(block, sems, rsems, 4, s, sib).start()
        elif n == 1:
            s = slot_of(yat(dy), c)
            ycopy(block, sems, rsems, 0, s, sib).wait_recv()
            ycopy(block, sems, rsems, 5, s, sib).start()
        else:
            s = slot_of(yat(2), c)
            ycopy(block, sems, rsems, 0, s, sib).wait_recv()
            ycopy(block, sems, rsems, 6, s, sib).start()

    def yfinish(block, sems, rsems):
        for n in range(4):
            s = slot_of(yat(n), 1 - c)
            ycopy(block, sems, rsems, 0, s, sib).wait_recv()

    def oblock(slot):
        t = (slot % 4) * 2 + slot // 4
        return GO.at[pl.ds(pl.multiple_of(t * 128, 128), 128)]

    def nblock(part):
        def view(slot):
            return NA.at[pl.ds(pl.multiple_of(slot * OWN, OWN), OWN), pl.ds(part * (D // 2), D // 2)]

        return view, nss.at[part], nrs.at[part]

    half_lane = lax.broadcasted_iota(jnp.int32, (HQ, 128), 1)

    def spread(half, q):
        qs = q.astype(F32) * (HEAD_DIM ** (-0.5))
        QZ[half, :HQ, :] = jnp.where(half_lane < HEAD_DIM, qs, 0.0).astype(BF)
        QZ[half, HQ:, :] = jnp.where(half_lane >= HEAD_DIM, qs, 0.0).astype(BF)

    def qcopy():
        return pltpu.make_async_remote_copy(
            src_ref=q_ref.at[pl.ds(HQ, HQ)], dst_ref=QR, send_sem=qsem.at[0], recv_sem=qsem.at[1],
            device_id=(ps, tp), device_id_type=MESH,
        )

    for cp in local[:3]:
        cp.wait()
    pl.semaphore_wait(bar, 19)
    qcopy().start()
    for p in KV:
        begin(p)
    local[4].wait()
    ybegin(oblock, oss, ors)
    spread(0, q_ref[:HQ, :])
    ACC[1] = jnp.zeros((2 * HQ, 256), F32)
    MX[1] = jnp.full((2 * HQ, 128), -1e30, F32)

    def scores(half, s, width, r0=0):
        kb = GK[pl.ds(pl.multiple_of(s * ROWS, ROWS), width), :]
        return lax.dot_general(QZ[half], kb, NT, preferred_element_type=F32)

    def values_of(s, width):
        vb = GV[pl.ds(pl.multiple_of(s * ROWS, ROWS), width), :]
        return jnp.concatenate([vb, jnp.ones((width, 128), BF)], axis=1)

    def attend(half, s, width, first_key, is_first):
        sc = scores(half, s, width)
        tops, wts = [], []
        for h in range(2):
            sh = sc[h * HQ : (h + 1) * HQ] - GG[s, h : h + 1, :width]
            if first_key is not None:
                row = lax.broadcasted_iota(jnp.int32, (HQ, width), 0) + first_key
                col = lax.broadcasted_iota(jnp.int32, (HQ, width), 1)
                sh = jnp.where(col <= row, sh, -1e30)
            top = jnp.max(sh, axis=1, keepdims=True)
            if is_first:
                top = jnp.broadcast_to(top, (HQ, 128))
            else:
                top = jnp.maximum(MX[half, h * HQ : (h + 1) * HQ, :], top)
            wts.append(jnp.exp(sh - jnp.concatenate([top] * (width // 128), axis=1)).astype(BF))
            tops.append(top)
        top = jnp.concatenate(tops, axis=0)
        pv = jnp.dot(jnp.concatenate(wts, axis=0), values_of(s, width), preferred_element_type=F32)
        if is_first:
            ACC[half] = pv
        else:
            fade = jnp.exp(MX[half] - top)
            ACC[half] = ACC[half] * jnp.concatenate([fade, fade], axis=1) + pv
        MX[half] = top

    attend(0, sp, HQ, 0, True)
    qcopy().wait_recv()
    spread(1, QR[...])
    for cp in local[5:7]:
        cp.wait()
    mine = pl.ds(pl.multiple_of(sp * 128, 128), 128)
    for j in range(5):
        GW[mine, j * 256 : j * 256 + 128] = wg_ref[:, j * 128 : (j + 1) * 128]
        GW[mine, j * 256 + 128 : (j + 1) * 256] = wu_ref[:, j * 128 : (j + 1) * 128]
    GW[mine, 1280:1408] = jnp.concatenate(
        [wg_ref[:, 640:], wu_ref[:, 640:], jnp.zeros((128, 32), BF)], axis=1
    )
    local[3].wait()
    for k in range(1, LOOK):
        for p in KV:
            serve(p, k)

    def step(k, _):
        @pl.when((k + LOOK < N_SP) & (k + LOOK > 0))
        def _():
            for p in KV:
                serve(p, k + LOOK)

        @pl.when(k == K_O1)
        def _():
            yserve(oblock, oss, ors, 0)
            yserve(oblock, oss, ors, 1)

        @pl.when(k == K_O2)
        def _():
            yserve(oblock, oss, ors, 2)

        @pl.when(k == K_W)
        def _():
            for p in WEIGHTS:
                begin_first(p)

        @pl.when(k == K_WS)
        def _():
            for p in WEIGHTS:
                serve_first(p, 1)
                serve_first(p, 3)

        s = spof(*offsets(k))

        @pl.when(s < sp)
        def _():
            attend(0, s, ROWS, None, False)

        @pl.when(s < ps)
        def _():
            attend(1, s, ROWS, None, False)

        @pl.when(s == ps)
        def _():
            attend(1, s, ROWS, HQ, False)

        return 0

    lax.fori_loop(0, N_SP, step, 0)

    for half in range(2):
        o0 = ACC[half, :HQ, :128] / ACC[half, :HQ, 128:]
        o1 = ACC[half, HQ:, :128] / ACC[half, HQ:, 128:]
        ATL[half * HQ : (half + 1) * HQ, :] = jnp.where(half_lane < HEAD_DIM, o0, o1).astype(BF)

    def acopy(i, dst, slot):
        return pltpu.make_async_remote_copy(
            src_ref=ATL.at[pl.ds(pl.multiple_of(dst * OWN, 32), OWN)],
            dst_ref=AT.at[:, pl.ds(pl.multiple_of(slot * 128, 128), 128)],
            send_sem=ass.at[i], recv_sem=ars.at[slot],
            device_id=(sp + (dst // 4) * (ps - sp), dst), device_id_type=MESH,
        )

    for i in range(1, 8):
        acopy(i, (tp + i) % 8, tp).start()

    @pl.when(tp >= 4)
    def _():
        acopy(0, tp, tp).start()

    @pl.when(tp < 4)
    def _():
        AT[:, pl.ds(pl.multiple_of(tp * 128, 128), 128)] = ATL[pl.ds(pl.multiple_of(tp * OWN, 32), OWN), :]

    for p in (3, 4):
        serve_first(p, 2)
        for da in (0, 1, 3, 2):
            send_second(p, da)
    yfinish(oblock, oss, ors)
    for cp in local[7:]:
        cp.wait()
    for i in range(1, 8):
        acopy(0, tp, (tp + i) % 8).wait_recv()

    @pl.when(tp >= 4)
    def _():
        acopy(0, tp, tp).wait_recv()

    NB = 512
    sq = jnp.zeros((OWN, 1), F32)
    for j in range(D // NB):
        pj = jnp.dot(AT[...], GO[:, j * NB : (j + 1) * NB], preferred_element_type=F32)
        mj = resid_ref[:, j * NB : (j + 1) * NB].astype(F32) + pj
        MIX[:, j * NB : (j + 1) * NB] = mj
        sq = sq + jnp.sum(mj * mj, axis=1, keepdims=True)
    inv = lax.rsqrt(sq * (1.0 / D) + 1e-6)
    own_slot = slot_of(y, c)
    NA[pl.ds(pl.multiple_of(own_slot * OWN, OWN), OWN), :] = (MIX[...] * inv * gain_ref[...]).astype(BF)
    for h in range(2):
        ybegin(*nblock(h))
    relay(3)
    for p in (5, 6):
        serve_first(p, 2)
        for da in (0, 1, 3, 2):
            send_second(p, da)
    relay(4)
    for n in range(2):
        for h in range(2):
            yserve(*nblock(h), n)
    relay(5)
    for h in range(2):
        yserve(*nblock(h), 2)
    relay(6)
    collect(3)
    collect(4)
    for h in range(2):
        yfinish(*nblock(h))

    def gu(j, _):
        col = pl.multiple_of(j * 256, 256)
        r = jnp.dot(NA[...], GW[:, pl.ds(col, 256)], preferred_element_type=F32)
        gt = r[:, :128]
        HID[:, pl.ds(pl.multiple_of(j * 128, 128), 128)] = (gt / (1.0 + jnp.exp(-gt)) * r[:, 128:]).astype(BF)
        return 0

    lax.fori_loop(0, 5, gu, 0)
    r = jnp.dot(NA[...], GW[:, 1280:1408], preferred_element_type=F32)
    gt = r[:, :48]
    HID[:, 640:688] = (gt / (1.0 + jnp.exp(-gt)) * r[:, 48:96]).astype(BF)
    collect(5)
    collect(6)

    half = 4 * OWN

    def scopy(j):
        view = (slice(None), pl.ds(j * NB, NB))
        return pltpu.make_async_remote_copy(
            src_ref=SB.at[view], dst_ref=RB.at[view], send_sem=bss.at[j], recv_sem=brs.at[j],
            device_id=(sp, sib), device_id_type=MESH,
        )

    def rcopy(n, j, to):
        view = (n, slice(None), pl.ds(j * NB, NB))
        return pltpu.make_async_remote_copy(
            src_ref=TB.at[view], dst_ref=RR.at[view], send_sem=css.at[n, j], recv_sem=crs.at[n, j],
            device_id=(sp, tpof(yat(to), c)), device_id_type=MESH,
        )

    def ocopy(j):
        view = (slice(None), pl.ds(j * NB, NB))
        return pltpu.make_async_copy(out_ref.at[view], out_hbm.at[view], osem.at[j])

    def both(n, j):
        view = (pl.ds(pl.multiple_of(yat(n) * OWN, OWN), OWN), slice(j * NB, (j + 1) * NB))
        return PA[view] + RB[view].astype(F32)

    NC = D // NB
    hs = HID[pl.ds(pl.multiple_of((1 - c) * half, half), half), :]
    ho = HID[pl.ds(pl.multiple_of(c * half, half), half), :]
    for j in range(NC):
        cols = slice(j * NB, (j + 1) * NB)
        SB[:, cols] = jnp.dot(hs, GD[:, cols], preferred_element_type=F32).astype(BF)
        scopy(j).start()
        PA[:, cols] = jnp.dot(ho, GD[:, cols], preferred_element_type=F32)
        if j > 0:
            scopy(j - 1).wait_recv()
            TB[0, :, (j - 1) * NB : j * NB] = both(2, j - 1).astype(BF)
            rcopy(0, j - 1, dy).start()
    scopy(NC - 1).wait_recv()
    TB[0, :, (NC - 1) * NB :] = both(2, NC - 1).astype(BF)
    rcopy(0, NC - 1, dy).start()
    for j in range(NC):
        cols = slice(j * NB, (j + 1) * NB)
        TB[1, :, cols] = both(-dy, j).astype(BF)
        rcopy(1, j, -dy).start()
    for j in range(NC):
        cols = slice(j * NB, (j + 1) * NB)
        rcopy(0, j, dy).wait_recv()
        TB[2, :, cols] = (both(dy, j) + RR[0, :, cols].astype(F32)).astype(BF)
        rcopy(2, j, dy).start()
    for j in range(NC):
        cols = slice(j * NB, (j + 1) * NB)
        rcopy(1, j, -dy).wait_recv()
        rcopy(2, j, dy).wait_recv()
        ffn = both(0, j) + RR[1, :, cols].astype(F32) + RR[2, :, cols].astype(F32)
        out_ref[:, cols] = (MIX[:, cols] + 0.5 * ffn).astype(BF)
        ocopy(j).start()

    for j in range(NC):
        for n in range(3):
            rcopy(n, j, dy).wait_send()
        scopy(j).wait_send()
    for i in range(1, 8):
        acopy(i, tp, tp).wait_send()

    @pl.when(tp >= 4)
    def _():
        acopy(0, tp, tp).wait_send()

    qcopy().wait_send()
    for j in range(NC):
        ocopy(j).wait()
    for i in range(7):
        ycopy(oblock, oss, ors, i, slot_of(y, c), sib).wait_send()
        for h in range(2):
            ycopy(*nblock(h), i, slot_of(y, c), sib).wait_send()
    for p in range(N_PIECE):

        def drain(i, _):
            copy(p, sp, i, sp).wait_send()
            return 0

        lax.fori_loop(0, 15, drain, 0)


def local(resid, queries, keys, values, cum_gate, out_weight, norm_gain, gate_weight, up_weight, down_weight):
    vm = pl.BlockSpec(memory_space=pltpu.VMEM)
    hbm = pl.BlockSpec(memory_space=pl.ANY)
    dma = pltpu.SemaphoreType.DMA
    V = pltpu.VMEM
    return pl.pallas_call(
        kernel,
        out_shape=jax.ShapeDtypeStruct((OWN, D), BF),
        in_specs=[vm] + [hbm] * 9,
        out_specs=hbm,
        scratch_shapes=[
            V((N_SP, 2, ROWS), F32),
            V((N_SP * ROWS, 128), BF),
            V((N_SP * ROWS, 128), BF),
            V((D, GUW), BF),
            V((FFW, D), BF),
            V((1024, D), BF),
            V((HQ, 128), BF),
            V((2, ROWS, 128), BF),
            V((2, ROWS, 256), F32),
            V((2, ROWS, 128), F32),
            V((ROWS, 128), BF),
            V((OWN, 1024), BF),
            V((OWN, D), F32),
            V((ROWS, D), BF),
            V((ROWS, FFW), BF),
            V((4 * OWN, D), BF),
            V((4 * OWN, D), BF),
            V((4 * OWN, D), F32),
            V((3, OWN, D), BF),
            V((3, OWN, D), BF),
            V((128, FFW), BF),
            V((128, FFW), BF),
            V((OWN, D), BF),
            V((1, D), F32),
            V((OWN, D), BF),
            dma((N_PIECE, N_SP)),
            dma((N_PIECE, 15)),
            dma((8,)),
            dma((7,)),
            dma((2, 8)),
            dma((2, 7)),
            dma((8,)),
            dma((8,)),
            dma((4,)),
            dma((4,)),
            dma((3, 4)),
            dma((3, 4)),
            dma((9,)),
            dma((2,)),
            dma((4,)),
        ],
        compiler_params=pltpu.CompilerParams(
            collective_id=0, has_side_effects=True, vmem_limit_bytes=64 * 1024 * 1024 - 128 * 1024
        ),
        name="layer",
    )(
        queries, keys, values, cum_gate.T, out_weight, gate_weight, up_weight, down_weight, resid,
        norm_gain.reshape(1, D),
    )


def solution(mesh):
    return jax.shard_map(
        local,
        mesh=mesh,
        in_specs=(
            P(("sp", "tp"), None),
            P("sp", "tp"),
            P("sp", "tp"),
            P("sp", "tp"),
            P("sp", "tp"),
            P("tp", None),
            P(),
            P("sp", "tp"),
            P("sp", "tp"),
            P("tp", "sp"),
        ),
        out_specs=P(("sp", "tp"), None),
        check_vma=False,
    )
```

```python
import functools

import jax
import jax.numpy as jnp
from jax import lax
from jax.experimental import pallas as pl
from jax.experimental.pallas import tpu as pltpu
from jax.sharding import PartitionSpec as P

HEAD_DIM = 64
ROWS = 768
OWN = 96
D = 2048
FFW = 688
N_SP = 16
HQ = ROWS // 2
QROWS = 384
AHEAD = 1
R5 = 0
R6 = 2
KV = (1, 2, 0)
LOOK = 1
K_O1 = 6
K_O2 = 10
K_W = 8
K_WS = 13
WEIGHTS = (3, 4, 5, 6)
BF = jnp.bfloat16
F32 = jnp.float32
MESH = pl.DeviceIdType.MESH
NT = (((1,), (1,)), ((), ()))

N_PIECE = 7
SIGN = (1, 1, -1, 1, -1, 1, -1)


WAVE = (
    (0, 0), (1, 0), (3, 0), (0, 1), (0, 3), (2, 0), (1, 1), (3, 1),
    (1, 3), (3, 3), (0, 2), (2, 1), (2, 3), (1, 2), (3, 2), (2, 2),
)


def offsets(k):
    if isinstance(k, int):
        return WAVE[k]
    da, db = jnp.int32(0), jnp.int32(0)
    for n in range(1, 16):
        da = jnp.where(k == n, WAVE[n][0], da)
        db = jnp.where(k == n, WAVE[n][1], db)
    return da, db


def kernel(
    q_in, k_ref, v_ref, g_ref, ow_ref, wg_ref, wu_ref, wd_ref, resid_in, gain_in,
    out_hbm,
    GG, GK, GV, GT, UT, GD, GO, QR, QZ, ACC, MX, ATL, AT, MIX, NA, HID, SB, RB, PA, TB, RR,
    q_ref, resid_ref, gain_ref, out_ref,
    rs, ss, ors, oss, nrs, nss, ars, ass, brs, bss, crs, css, lsem, qsem, osem,
):
    sp = lax.axis_index("sp")
    tp = lax.axis_index("tp")
    c = tp % 2
    y = tp // 2
    z = sp // 4
    x = sp % 4
    a = z + c * (x - z)
    b = x + c * (z - x)

    def spof(da, db):
        return ((a + da + 4) % 4) * (4 - 3 * c) + ((b + db + 4) % 4) * (1 + 3 * c)

    def tpof(yy, cc):
        return yy * 2 + cc

    sib = tpof(y, 1 - c)
    ps = N_SP - 1 - sp

    bar = pltpu.get_barrier_semaphore()
    for da, db in ((1, 0), (3, 0), (0, 1), (0, 3)):
        pl.semaphore_signal(bar, inc=1, device_id=(spof(da, db), tp), device_id_type=MESH)
    for i in range(8):
        if i:
            pl.semaphore_signal(bar, inc=1, device_id=(sp, (tp + i) % 8), device_id_type=MESH)
        pl.semaphore_signal(bar, inc=1, device_id=(ps, (tp + i) % 8), device_id_type=MESH)

    def part(p, s):
        if p == 0:
            return GG.at[s]
        if p == 1:
            return GK.at[pl.ds(pl.multiple_of(s * ROWS, ROWS), ROWS)]
        if p == 2:
            return GV.at[pl.ds(pl.multiple_of(s * ROWS, ROWS), ROWS)]
        if p == 3:
            return GT.at[:, pl.ds(pl.multiple_of(s * 128, 128), 128)]
        if p == 4:
            return UT.at[:, pl.ds(pl.multiple_of(s * 128, 128), 128)]
        if p == 5:
            return GD.at[pl.ds(0, 352), pl.ds(pl.multiple_of(s * 128, 128), 128)]
        return GD.at[pl.ds(352, 336), pl.ds(pl.multiple_of(s * 128, 128), 128)]

    local = [
        pltpu.make_async_copy(g_ref, part(0, sp), lsem.at[0]),
        pltpu.make_async_copy(k_ref, part(1, sp), lsem.at[1]),
        pltpu.make_async_copy(v_ref, part(2, sp), lsem.at[2]),
        pltpu.make_async_copy(wd_ref, GD.at[:, pl.ds(pl.multiple_of(sp * 128, 128), 128)], lsem.at[3]),
        pltpu.make_async_copy(ow_ref, GO.at[pl.ds(pl.multiple_of(tp * 128, 128), 128)], lsem.at[4]),
        pltpu.make_async_copy(wg_ref, part(3, sp), lsem.at[5]),
        pltpu.make_async_copy(wu_ref, part(4, sp), lsem.at[6]),
        pltpu.make_async_copy(resid_in, resid_ref, lsem.at[7]),
        pltpu.make_async_copy(gain_in, gain_ref, lsem.at[8]),
    ]
    q_local = pltpu.make_async_copy(q_in, q_ref, lsem.at[9])
    for cp in [q_local] + local:
        cp.start()

    def copy(p, s, idx, dst):
        return pltpu.make_async_remote_copy(
            src_ref=part(p, s), dst_ref=part(p, s), send_sem=ss.at[p, idx], recv_sem=rs.at[p, s],
            device_id=(dst, tp), device_id_type=MESH,
        )

    def begin_first(p):
        copy(p, sp, 0, spof(1, 0)).start()
        copy(p, sp, 1, spof(3, 0)).start()

    def send_second(p, da):
        s = spof(da, 0)
        copy(p, s, 2 + 2 * da, spof(0, 1)).start()
        copy(p, s, 3 + 2 * da, spof(0, 3)).start()

    def begin(p):
        begin_first(p)
        send_second(p, 0)

    def serve_first(p, da):
        s = spof(da, 0)
        copy(p, s, 0, sp).wait_recv()
        d = SIGN[p]
        if da == (4 - d) % 4:
            copy(p, s, 10, spof(d, 0)).start()

    def onward(p, da):
        return SIGN[p] * (1 - 2 * (da % 2))

    def relay(p):
        for da in (0, 1, 3, 2):
            d = onward(p, da)
            s = spof(da, 4 - d)
            copy(p, s, 0, sp).wait_recv()
            copy(p, s, 11 + da, spof(0, d)).start()

    def collect(p):
        for da in (0, 1, 3, 2):
            for db in (4 + onward(p, da), 2):
                copy(p, spof(da, db), 0, sp).wait_recv()

    def serve(p, k):
        da, db = offsets(k)
        s = spof(da, db)
        copy(p, s, 0, sp).wait_recv()
        d = SIGN[p]
        back = (4 - d) % 4

        @pl.when((db == 0) & (da == back))
        def _():
            copy(p, s, 10, spof(d, 0)).start()

        @pl.when(db == 0)
        def _():
            copy(p, s, 2 + 2 * da, spof(0, 1)).start()
            copy(p, s, 3 + 2 * da, spof(0, 3)).start()

        @pl.when(db == back)
        def _():
            copy(p, s, 11 + da, spof(0, d)).start()

    dy = 1 - 2 * c

    def yat(n):
        return (y + n + 4) % 4

    def ycopy(block, sems, rsems, idx, slot, dst):
        return pltpu.make_async_remote_copy(
            src_ref=block(slot), dst_ref=block(slot), send_sem=sems.at[idx], recv_sem=rsems.at[slot],
            device_id=(sp, dst), device_id_type=MESH,
        )

    def slot_of(yy, cc):
        return cc * 4 + yy

    def ybegin(block, sems, rsems):
        own = slot_of(y, c)
        ycopy(block, sems, rsems, 0, own, tpof(yat(dy), c)).start()
        ycopy(block, sems, rsems, 1, own, tpof(yat(-dy), c)).start()
        ycopy(block, sems, rsems, 2, own, sib).start()

    def yserve(block, sems, rsems, n):
        if n == 0:
            s = slot_of(yat(-dy), c)
            ycopy(block, sems, rsems, 0, s, sib).wait_recv()
            ycopy(block, sems, rsems, 3, s, tpof(yat(dy), c)).start()
            ycopy(block, sems, rsems, 4, s, sib).start()
        elif n == 1:
            s = slot_of(yat(dy), c)
            ycopy(block, sems, rsems, 0, s, sib).wait_recv()
            ycopy(block, sems, rsems, 5, s, sib).start()
        else:
            s = slot_of(yat(2), c)
            ycopy(block, sems, rsems, 0, s, sib).wait_recv()
            ycopy(block, sems, rsems, 6, s, sib).start()

    def yfinish(block, sems, rsems):
        for n in range(4):
            s = slot_of(yat(n), 1 - c)
            ycopy(block, sems, rsems, 0, s, sib).wait_recv()

    def oblock(slot):
        t = (slot % 4) * 2 + slot // 4
        return GO.at[pl.ds(pl.multiple_of(t * 128, 128), 128)]

    def nblock(part):
        def view(slot):
            return NA.at[pl.ds(pl.multiple_of(slot * OWN, OWN), OWN), pl.ds(part * (D // 2), D // 2)]

        return view, nss.at[part], nrs.at[part]

    half_lane = lax.broadcasted_iota(jnp.int32, (HQ, 128), 1)

    def spread(half, q):
        qs = q.astype(F32) * (HEAD_DIM ** (-0.5))
        QZ[half, :HQ, :] = jnp.where(half_lane < HEAD_DIM, qs, 0.0).astype(BF)
        QZ[half, HQ:, :] = jnp.where(half_lane >= HEAD_DIM, qs, 0.0).astype(BF)

    def qcopy():
        return pltpu.make_async_remote_copy(
            src_ref=q_ref.at[pl.ds(HQ, HQ)], dst_ref=QR, send_sem=qsem.at[0], recv_sem=qsem.at[1],
            device_id=(ps, tp), device_id_type=MESH,
        )

    for cp in [q_local] + local[:3]:
        cp.wait()
    pl.semaphore_wait(bar, 19)
    qcopy().start()
    for p in KV:
        begin(p)
    local[4].wait()
    ybegin(oblock, oss, ors)
    spread(0, q_ref[:HQ, :])
    ACC[1] = jnp.zeros((2 * HQ, 256), F32)
    MX[1] = jnp.full((2 * HQ, 128), -1e30, F32)

    def values_of(s, width):
        vb = GV[pl.ds(pl.multiple_of(s * ROWS, ROWS), width), :]
        return jnp.concatenate([vb, jnp.ones((width, 128), BF)], axis=1)

    def attend(half, s, width, first_key, is_first):
        kb = GK[pl.ds(pl.multiple_of(s * ROWS, ROWS), width), :]
        vb = values_of(s, width)
        count = 2 * HQ // QROWS

        def score(n):
            return lax.dot_general(
                QZ[half, n * QROWS : (n + 1) * QROWS, :], kb, NT, preferred_element_type=F32
            )

        def finish(n, sc):
            h, r0 = divmod(n * QROWS, HQ)
            rows = slice(n * QROWS, (n + 1) * QROWS)
            sh = sc - GG[s, h : h + 1, :width]
            if first_key is not None:
                row = lax.broadcasted_iota(jnp.int32, (QROWS, width), 0) + (first_key + r0)
                col = lax.broadcasted_iota(jnp.int32, (QROWS, width), 1)
                sh = jnp.where(col <= row, sh, -1e30)
            top = jnp.max(sh, axis=1, keepdims=True)
            if is_first:
                top = jnp.broadcast_to(top, (QROWS, 128))
            else:
                old = MX[half, rows, :]
                top = jnp.maximum(old, top)
            wt = jnp.exp(sh - jnp.concatenate([top] * (width // 128), axis=1)).astype(BF)
            pv = jnp.dot(wt, vb, preferred_element_type=F32)
            if is_first:
                ACC[half, rows, :] = pv
            else:
                fade = jnp.exp(old - top)
                ACC[half, rows, :] = ACC[half, rows, :] * jnp.concatenate([fade, fade], axis=1) + pv
            MX[half, rows, :] = top

        held = [score(n) for n in range(AHEAD)]
        for n in range(count):
            if n + AHEAD < count:
                held.append(score(n + AHEAD))
            finish(n, held[n])

    attend(0, sp, HQ, 0, True)
    qcopy().wait_recv()
    spread(1, QR[...])
    for cp in local[5:7]:
        cp.wait()
    local[3].wait()
    for k in range(1, LOOK):
        for p in KV:
            serve(p, k)

    def step(k, _):
        @pl.when((k + LOOK < N_SP) & (k + LOOK > 0))
        def _():
            for p in KV:
                serve(p, k + LOOK)

        @pl.when(k == K_O1)
        def _():
            yserve(oblock, oss, ors, 0)
            yserve(oblock, oss, ors, 1)

        @pl.when(k == K_O2)
        def _():
            yserve(oblock, oss, ors, 2)

        @pl.when(k == K_W)
        def _():
            for p in WEIGHTS:
                begin_first(p)

        @pl.when(k == K_WS)
        def _():
            for p in WEIGHTS:
                serve_first(p, 1)
                serve_first(p, 3)

        s = spof(*offsets(k))

        @pl.when(s < sp)
        def _():
            attend(0, s, ROWS, None, False)

        @pl.when(s < ps)
        def _():
            attend(1, s, ROWS, None, False)

        @pl.when(s == ps)
        def _():
            attend(1, s, ROWS, HQ, False)

        return 0

    lax.fori_loop(0, N_SP, step, 0)

    for half in range(2):
        o0 = ACC[half, :HQ, :128] / ACC[half, :HQ, 128:]
        o1 = ACC[half, HQ:, :128] / ACC[half, HQ:, 128:]
        ATL[half * HQ : (half + 1) * HQ, :] = jnp.where(half_lane < HEAD_DIM, o0, o1).astype(BF)

    def acopy(i, dst, slot):
        return pltpu.make_async_remote_copy(
            src_ref=ATL.at[pl.ds(pl.multiple_of(dst * OWN, 32), OWN)],
            dst_ref=AT.at[:, pl.ds(pl.multiple_of(slot * 128, 128), 128)],
            send_sem=ass.at[i], recv_sem=ars.at[slot],
            device_id=(sp + (dst // 4) * (ps - sp), dst), device_id_type=MESH,
        )

    for i in range(1, 8):
        acopy(i, (tp + i) % 8, tp).start()

    @pl.when(tp >= 4)
    def _():
        acopy(0, tp, tp).start()

    @pl.when(tp < 4)
    def _():
        AT[:, pl.ds(pl.multiple_of(tp * 128, 128), 128)] = ATL[pl.ds(pl.multiple_of(tp * OWN, 32), OWN), :]

    for p in (3, 4):
        serve_first(p, 2)
        for da in (0, 1, 3, 2):
            send_second(p, da)
    yfinish(oblock, oss, ors)
    for cp in local[7:]:
        cp.wait()
    for i in range(1, 8):
        acopy(0, tp, (tp + i) % 8).wait_recv()

    @pl.when(tp >= 4)
    def _():
        acopy(0, tp, tp).wait_recv()

    NB = 512
    sq = jnp.zeros((OWN, 1), F32)
    for j in range(D // NB):
        pj = jnp.dot(AT[...], GO[:, j * NB : (j + 1) * NB], preferred_element_type=F32)
        mj = resid_ref[:, j * NB : (j + 1) * NB].astype(F32) + pj
        MIX[:, j * NB : (j + 1) * NB] = mj
        sq = sq + jnp.sum(mj * mj, axis=1, keepdims=True)
    inv = lax.rsqrt(sq * (1.0 / D) + 1e-6)
    own_slot = slot_of(y, c)
    NA[pl.ds(pl.multiple_of(own_slot * OWN, OWN), OWN), :] = (MIX[...] * inv * gain_ref[...]).astype(BF)
    for h in range(2):
        ybegin(*nblock(h))
    relay(3)
    relay(4)
    for p in (5, 6):
        serve_first(p, 2)
        for da in (0, 1, 3, 2):
            send_second(p, da)
    for n in range(2):
        for h in range(2):
            yserve(*nblock(h), n)
    for h in range(2):
        yserve(*nblock(h), 2)
    collect(3)
    collect(4)
    for h in range(2):
        yfinish(*nblock(h))

    def gu(j, _):
        @pl.when(j == R5)
        def _():
            relay(5)

        @pl.when(j == R6)
        def _():
            relay(6)

        gate_up(pl.multiple_of(j * 128, 128), 128)
        return 0

    def gate_up(c0, n):
        rows = pl.ds(c0, n)
        r = lax.dot_general(
            NA[...], jnp.concatenate([GT[rows, :], UT[rows, :]], axis=0), NT, preferred_element_type=F32
        )
        gt = r[:, :n]
        HID[:, rows] = (gt / (1.0 + jnp.exp(-gt)) * r[:, n:]).astype(BF)

    lax.fori_loop(0, 5, gu, 0)
    gate_up(640, 48)
    collect(5)
    collect(6)

    half = 4 * OWN

    def scopy(j):
        view = (slice(None), pl.ds(j * NB, NB))
        return pltpu.make_async_remote_copy(
            src_ref=SB.at[view], dst_ref=RB.at[view], send_sem=bss.at[j], recv_sem=brs.at[j],
            device_id=(sp, sib), device_id_type=MESH,
        )

    def rcopy(n, j, to):
        view = (n, slice(None), pl.ds(j * NB, NB))
        return pltpu.make_async_remote_copy(
            src_ref=TB.at[view], dst_ref=RR.at[view], send_sem=css.at[n, j], recv_sem=crs.at[n, j],
            device_id=(sp, tpof(yat(to), c)), device_id_type=MESH,
        )

    def ocopy(j):
        view = (slice(None), pl.ds(j * NB, NB))
        return pltpu.make_async_copy(out_ref.at[view], out_hbm.at[view], osem.at[j])

    def both(n, j):
        view = (pl.ds(pl.multiple_of(yat(n) * OWN, OWN), OWN), slice(j * NB, (j + 1) * NB))
        return PA[view] + RB[view].astype(F32)

    NC = D // NB
    hs = HID[pl.ds(pl.multiple_of((1 - c) * half, half), half), :]
    ho = HID[pl.ds(pl.multiple_of(c * half, half), half), :]
    for j in range(NC):
        cols = slice(j * NB, (j + 1) * NB)
        SB[:, cols] = jnp.dot(hs, GD[:, cols], preferred_element_type=F32).astype(BF)
        scopy(j).start()
        PA[:, cols] = jnp.dot(ho, GD[:, cols], preferred_element_type=F32)
        if j > 0:
            scopy(j - 1).wait_recv()
            TB[0, :, (j - 1) * NB : j * NB] = both(2, j - 1).astype(BF)
            rcopy(0, j - 1, dy).start()
    scopy(NC - 1).wait_recv()
    TB[0, :, (NC - 1) * NB :] = both(2, NC - 1).astype(BF)
    rcopy(0, NC - 1, dy).start()
    for j in range(NC):
        cols = slice(j * NB, (j + 1) * NB)
        TB[1, :, cols] = both(-dy, j).astype(BF)
        rcopy(1, j, -dy).start()
    for p in range(N_PIECE):

        def drain(i, _):
            copy(p, sp, i, sp).wait_send()
            return 0

        lax.fori_loop(0, 15, drain, 0)
    for i in range(7):
        ycopy(oblock, oss, ors, i, slot_of(y, c), sib).wait_send()
        for h in range(2):
            ycopy(*nblock(h), i, slot_of(y, c), sib).wait_send()
    for i in range(1, 8):
        acopy(i, tp, tp).wait_send()

    @pl.when(tp >= 4)
    def _():
        acopy(0, tp, tp).wait_send()

    qcopy().wait_send()
    for j in range(NC):
        cols = slice(j * NB, (j + 1) * NB)
        rcopy(0, j, dy).wait_recv()
        TB[2, :, cols] = (both(dy, j) + RR[0, :, cols].astype(F32)).astype(BF)
        rcopy(2, j, dy).start()
    for j in range(NC):
        cols = slice(j * NB, (j + 1) * NB)
        rcopy(1, j, -dy).wait_recv()
        rcopy(2, j, dy).wait_recv()
        ffn = both(0, j) + RR[1, :, cols].astype(F32) + RR[2, :, cols].astype(F32)
        out_ref[:, cols] = (MIX[:, cols] + 0.5 * ffn).astype(BF)
        ocopy(j).start()

    for j in range(NC):
        for n in range(3):
            rcopy(n, j, dy).wait_send()
        scopy(j).wait_send()
    for j in range(NC):
        ocopy(j).wait()


def local(resid, queries, keys, values, cum_gate, out_weight, norm_gain, gate_weight, up_weight, down_weight):
    hbm = pl.BlockSpec(memory_space=pl.ANY)
    dma = pltpu.SemaphoreType.DMA
    V = pltpu.VMEM
    return pl.pallas_call(
        kernel,
        out_shape=jax.ShapeDtypeStruct((OWN, D), BF),
        in_specs=[hbm] * 10,
        out_specs=hbm,
        scratch_shapes=[
            V((N_SP, 2, ROWS), F32),
            V((N_SP * ROWS, 128), BF),
            V((N_SP * ROWS, 128), BF),
            V((FFW, D), BF),
            V((FFW, D), BF),
            V((FFW, D), BF),
            V((1024, D), BF),
            V((HQ, 128), BF),
            V((2, ROWS, 128), BF),
            V((2, ROWS, 256), F32),
            V((2, ROWS, 128), F32),
            V((ROWS, 128), BF),
            V((OWN, 1024), BF),
            V((OWN, D), F32),
            V((ROWS, D), BF),
            V((ROWS, FFW), BF),
            V((4 * OWN, D), BF),
            V((4 * OWN, D), BF),
            V((4 * OWN, D), F32),
            V((3, OWN, D), BF),
            V((3, OWN, D), BF),
            V((ROWS, 128), BF),
            V((OWN, D), BF),
            V((1, D), F32),
            V((OWN, D), BF),
            dma((N_PIECE, N_SP)),
            dma((N_PIECE, 15)),
            dma((8,)),
            dma((7,)),
            dma((2, 8)),
            dma((2, 7)),
            dma((8,)),
            dma((8,)),
            dma((4,)),
            dma((4,)),
            dma((3, 4)),
            dma((3, 4)),
            dma((10,)),
            dma((2,)),
            dma((4,)),
        ],
        compiler_params=pltpu.CompilerParams(
            collective_id=0, has_side_effects=True, vmem_limit_bytes=64 * 1024 * 1024 - 128 * 1024
        ),
        name="layer",
    )(
        queries, keys, values, cum_gate.T, out_weight, gate_weight.T, up_weight.T, down_weight, resid,
        norm_gain.reshape(1, D),
    )


def solution(mesh):
    return jax.shard_map(
        local,
        mesh=mesh,
        in_specs=(
            P(("sp", "tp"), None),
            P("sp", "tp"),
            P("sp", "tp"),
            P("sp", "tp"),
            P("sp", "tp"),
            P("tp", None),
            P(),
            P("sp", "tp"),
            P("sp", "tp"),
            P("tp", "sp"),
        ),
        out_specs=P(("sp", "tp"), None),
        check_vma=False,
    )
```

```python
import functools

import jax
import jax.numpy as jnp
from jax import lax
from jax.experimental import pallas as pl
from jax.experimental.pallas import tpu as pltpu
from jax.sharding import PartitionSpec as P

HEAD_DIM = 64
ROWS = 768
OWN = 96
D = 2048
FFW = 688
N_SP = 16
NB = 256
NC = D // NB
HQ = ROWS // 2
QROWS = 384
AHEAD = 1
R5 = 0
R6 = 2
KV = (1, 2, 0)
LOOK = 1
EARLY = (0,)
MIXED = False
K_O1 = 6
K_O2 = 10
K_W = 8
K_WS = 13
WEIGHTS = (3, 4, 5, 6)
BF = jnp.bfloat16
F32 = jnp.float32
MESH = pl.DeviceIdType.MESH
NT = (((1,), (1,)), ((), ()))

N_PIECE = 7
SIGN = (1, 1, -1, 1, -1, 1, -1)


WAVE = (
    (0, 0), (1, 0), (3, 0), (0, 1), (0, 3), (2, 0), (1, 1), (3, 1),
    (1, 3), (3, 3), (0, 2), (2, 1), (2, 3), (1, 2), (3, 2), (2, 2),
)


def offsets(k):
    if isinstance(k, int):
        return WAVE[k]
    da, db = jnp.int32(0), jnp.int32(0)
    for n in range(1, 16):
        da = jnp.where(k == n, WAVE[n][0], da)
        db = jnp.where(k == n, WAVE[n][1], db)
    return da, db


def kernel(
    q_in, k_ref, v_ref, g_ref, ow_ref, wg_ref, wu_ref, wd_ref, resid_in, gain_in,
    out_hbm,
    GG, GK, GV, GT, UT, GD, GO, QR, QZ, ACC, MX, ATL, AT, MIX, NA, HID, SB, RB, PA, TB, RR,
    q_ref, resid_ref, gain_ref, out_ref,
    rs, ss, ors, oss, nrs, nss, ars, ass, brs, bss, crs, css, lsem, qsem, osem,
):
    sp = lax.axis_index("sp")
    tp = lax.axis_index("tp")
    c = tp % 2
    y = tp // 2
    z = sp // 4
    x = sp % 4
    a = z + c * (x - z)
    b = x + c * (z - x)

    def spof(da, db):
        return ((a + da + 4) % 4) * (4 - 3 * c) + ((b + db + 4) % 4) * (1 + 3 * c)

    def tpof(yy, cc):
        return yy * 2 + cc

    sib = tpof(y, 1 - c)
    ps = N_SP - 1 - sp

    bar = pltpu.get_barrier_semaphore()
    for da, db in ((1, 0), (3, 0), (0, 1), (0, 3)):
        pl.semaphore_signal(bar, inc=1, device_id=(spof(da, db), tp), device_id_type=MESH)
    for i in range(8):
        if i:
            pl.semaphore_signal(bar, inc=1, device_id=(sp, (tp + i) % 8), device_id_type=MESH)
        pl.semaphore_signal(bar, inc=1, device_id=(ps, (tp + i) % 8), device_id_type=MESH)

    def part(p, s):
        if p == 0:
            return GG.at[s]
        if p == 1:
            return GK.at[pl.ds(pl.multiple_of(s * ROWS, ROWS), ROWS)]
        if p == 2:
            return GV.at[pl.ds(pl.multiple_of(s * ROWS, ROWS), ROWS)]
        if p == 3:
            return GT.at[:, pl.ds(pl.multiple_of(s * 128, 128), 128)]
        if p == 4:
            return UT.at[:, pl.ds(pl.multiple_of(s * 128, 128), 128)]
        if p == 5:
            return GD.at[pl.ds(0, 352), pl.ds(pl.multiple_of(s * 128, 128), 128)]
        return GD.at[pl.ds(352, 336), pl.ds(pl.multiple_of(s * 128, 128), 128)]

    local = [
        pltpu.make_async_copy(g_ref, part(0, sp), lsem.at[0]),
        pltpu.make_async_copy(k_ref, part(1, sp), lsem.at[1]),
        pltpu.make_async_copy(v_ref, part(2, sp), lsem.at[2]),
        pltpu.make_async_copy(wd_ref, GD.at[:, pl.ds(pl.multiple_of(sp * 128, 128), 128)], lsem.at[3]),
        pltpu.make_async_copy(ow_ref, GO.at[pl.ds(pl.multiple_of(tp * 128, 128), 128)], lsem.at[4]),
        pltpu.make_async_copy(wg_ref, part(3, sp), lsem.at[5]),
        pltpu.make_async_copy(wu_ref, part(4, sp), lsem.at[6]),
        pltpu.make_async_copy(resid_in, resid_ref, lsem.at[7]),
        pltpu.make_async_copy(gain_in, gain_ref, lsem.at[8]),
    ]
    q_local = pltpu.make_async_copy(q_in, q_ref, lsem.at[9])
    for cp in [q_local] + local:
        cp.start()

    def copy(p, s, idx, dst):
        return pltpu.make_async_remote_copy(
            src_ref=part(p, s), dst_ref=part(p, s), send_sem=ss.at[p, idx], recv_sem=rs.at[p, s],
            device_id=(dst, tp), device_id_type=MESH,
        )

    def begin_first(p):
        copy(p, sp, 0, spof(1, 0)).start()
        copy(p, sp, 1, spof(3, 0)).start()

    def send_second(p, da):
        s = spof(da, 0)
        copy(p, s, 2 + 2 * da, spof(0, 1)).start()
        copy(p, s, 3 + 2 * da, spof(0, 3)).start()

    def begin(p):
        begin_first(p)
        send_second(p, 0)

    def serve_first(p, da):
        s = spof(da, 0)
        copy(p, s, 0, sp).wait_recv()
        d = SIGN[p]
        if da == (4 - d) % 4:
            copy(p, s, 10, spof(d, 0)).start()

    def onward(p, da):
        return SIGN[p] * (1 - 2 * (da % 2))

    def relay(p):
        for da in (0, 1, 3, 2):
            d = onward(p, da)
            s = spof(da, 4 - d)
            copy(p, s, 0, sp).wait_recv()
            copy(p, s, 11 + da, spof(0, d)).start()

    def collect(p):
        for da in (0, 1, 3, 2):
            for db in (4 + onward(p, da), 2):
                copy(p, spof(da, db), 0, sp).wait_recv()

    def serve(p, k):
        da, db = offsets(k)
        s = spof(da, db)
        copy(p, s, 0, sp).wait_recv()
        d = SIGN[p]
        back = (4 - d) % 4

        @pl.when((db == 0) & (da == back))
        def _():
            copy(p, s, 10, spof(d, 0)).start()

        @pl.when(db == 0)
        def _():
            copy(p, s, 2 + 2 * da, spof(0, 1)).start()
            copy(p, s, 3 + 2 * da, spof(0, 3)).start()

        @pl.when(db == back)
        def _():
            copy(p, s, 11 + da, spof(0, d)).start()

    dy = 1 - 2 * c

    def yat(n):
        return (y + n + 4) % 4

    def ycopy(block, sems, rsems, idx, slot, dst):
        return pltpu.make_async_remote_copy(
            src_ref=block(slot), dst_ref=block(slot), send_sem=sems.at[idx], recv_sem=rsems.at[slot],
            device_id=(sp, dst), device_id_type=MESH,
        )

    def slot_of(yy, cc):
        return cc * 4 + yy

    def ybegin(block, sems, rsems):
        own = slot_of(y, c)
        ycopy(block, sems, rsems, 0, own, tpof(yat(dy), c)).start()
        ycopy(block, sems, rsems, 1, own, tpof(yat(-dy), c)).start()
        ycopy(block, sems, rsems, 2, own, sib).start()

    def yserve(block, sems, rsems, n):
        if n == 0:
            s = slot_of(yat(-dy), c)
            ycopy(block, sems, rsems, 0, s, sib).wait_recv()
            ycopy(block, sems, rsems, 3, s, tpof(yat(dy), c)).start()
            ycopy(block, sems, rsems, 4, s, sib).start()
        elif n == 1:
            s = slot_of(yat(dy), c)
            ycopy(block, sems, rsems, 0, s, sib).wait_recv()
            ycopy(block, sems, rsems, 5, s, sib).start()
        else:
            s = slot_of(yat(2), c)
            ycopy(block, sems, rsems, 0, s, sib).wait_recv()
            ycopy(block, sems, rsems, 6, s, sib).start()

    def yfinish(block, sems, rsems):
        for n in range(4):
            s = slot_of(yat(n), 1 - c)
            ycopy(block, sems, rsems, 0, s, sib).wait_recv()

    def oblock(slot):
        t = (slot % 4) * 2 + slot // 4
        return GO.at[pl.ds(pl.multiple_of(t * 128, 128), 128)]

    def nblock(part):
        def view(slot):
            return NA.at[pl.ds(pl.multiple_of(slot * OWN, OWN), OWN), pl.ds(part * (D // 2), D // 2)]

        return view, nss.at[part], nrs.at[part]

    half_lane = lax.broadcasted_iota(jnp.int32, (HQ, 128), 1)

    def spread(half, q):
        qs = q.astype(F32) * (HEAD_DIM ** (-0.5))
        QZ[half, :HQ, :] = jnp.where(half_lane < HEAD_DIM, qs, 0.0).astype(BF)
        QZ[half, HQ:, :] = jnp.where(half_lane >= HEAD_DIM, qs, 0.0).astype(BF)

    def qcopy():
        return pltpu.make_async_remote_copy(
            src_ref=q_ref.at[pl.ds(HQ, HQ)], dst_ref=QR, send_sem=qsem.at[0], recv_sem=qsem.at[1],
            device_id=(ps, tp), device_id_type=MESH,
        )

    for cp in [q_local] + local[:3]:
        cp.wait()
    pl.semaphore_wait(bar, 19)
    qcopy().start()
    for p in KV:
        begin_first(p)
        send_second(p, 0)
    local[4].wait()
    ybegin(oblock, oss, ors)
    spread(0, q_ref[:HQ, :])
    ACC[1] = jnp.zeros((2 * HQ, 256), F32)
    MX[1] = jnp.full((2 * HQ, 128), -1e30, F32)

    def values_of(s, width):
        vb = GV[pl.ds(pl.multiple_of(s * ROWS, ROWS), width), :]
        return jnp.concatenate([vb, jnp.ones((width, 128), BF)], axis=1)

    def attend(half, s, width, first_key, is_first):
        kb = GK[pl.ds(pl.multiple_of(s * ROWS, ROWS), width), :]
        vb = values_of(s, width)
        count = 2 * HQ // QROWS

        def score(n):
            return lax.dot_general(
                QZ[half, n * QROWS : (n + 1) * QROWS, :], kb, NT, preferred_element_type=F32
            )

        def finish(n, sc):
            h, r0 = divmod(n * QROWS, HQ)
            rows = slice(n * QROWS, (n + 1) * QROWS)
            sh = sc - GG[s, h : h + 1, :width]
            if first_key is not None:
                row = lax.broadcasted_iota(jnp.int32, (QROWS, width), 0) + (first_key + r0)
                col = lax.broadcasted_iota(jnp.int32, (QROWS, width), 1)
                sh = jnp.where(col <= row, sh, -1e30)
            top = jnp.max(sh, axis=1, keepdims=True)
            if is_first:
                top = jnp.broadcast_to(top, (QROWS, 128))
            else:
                old = MX[half, rows, :]
                top = jnp.maximum(old, top)
            wt = jnp.exp(sh - jnp.concatenate([top] * (width // 128), axis=1)).astype(BF)
            pv = jnp.dot(wt, vb, preferred_element_type=F32)
            if is_first:
                ACC[half, rows, :] = pv
            else:
                fade = jnp.exp(old - top)
                ACC[half, rows, :] = ACC[half, rows, :] * jnp.concatenate([fade, fade], axis=1) + pv
            MX[half, rows, :] = top

        held = [score(n) for n in range(AHEAD)]
        for n in range(count):
            if n + AHEAD < count:
                held.append(score(n + AHEAD))
            finish(n, held[n])

    attend(0, sp, HQ, 0, True)
    qcopy().wait_recv()
    spread(1, QR[...])
    for cp in local[5:7]:
        cp.wait()
    local[3].wait()
    for k in range(1, LOOK):
        for p in KV:
            serve(p, k)

    def step(k, _):
        @pl.when((k + LOOK < N_SP) & (k + LOOK > 0))
        def _():
            for p in KV:
                serve(p, k + LOOK)

        @pl.when(k == K_O1)
        def _():
            yserve(oblock, oss, ors, 0)
            yserve(oblock, oss, ors, 1)

        @pl.when(k == K_O2)
        def _():
            yserve(oblock, oss, ors, 2)

        @pl.when(k == K_W)
        def _():
            for p in WEIGHTS:
                begin_first(p)

        @pl.when(k == K_WS)
        def _():
            for p in WEIGHTS:
                serve_first(p, 1)
                serve_first(p, 3)
                if p < 5:
                    for da in EARLY:
                        send_second(p, da)

        s = spof(*offsets(k))

        @pl.when(s < sp)
        def _():
            attend(0, s, ROWS, None, False)

        @pl.when(s < ps)
        def _():
            attend(1, s, ROWS, None, False)

        @pl.when(s == ps)
        def _():
            attend(1, s, ROWS, HQ, False)

        return 0

    lax.fori_loop(0, N_SP, step, 0)

    for half in range(2):
        o0 = ACC[half, :HQ, :128] / ACC[half, :HQ, 128:]
        o1 = ACC[half, HQ:, :128] / ACC[half, HQ:, 128:]
        ATL[half * HQ : (half + 1) * HQ, :] = jnp.where(half_lane < HEAD_DIM, o0, o1).astype(BF)

    def acopy(i, dst, slot):
        return pltpu.make_async_remote_copy(
            src_ref=ATL.at[pl.ds(pl.multiple_of(dst * OWN, 32), OWN)],
            dst_ref=AT.at[:, pl.ds(pl.multiple_of(slot * 128, 128), 128)],
            send_sem=ass.at[i], recv_sem=ars.at[slot],
            device_id=(sp + (dst // 4) * (ps - sp), dst), device_id_type=MESH,
        )

    for i in range(1, 8):
        acopy(i, (tp + i) % 8, tp).start()

    @pl.when(tp >= 4)
    def _():
        acopy(0, tp, tp).start()

    @pl.when(tp < 4)
    def _():
        AT[:, pl.ds(pl.multiple_of(tp * 128, 128), 128)] = ATL[pl.ds(pl.multiple_of(tp * OWN, 32), OWN), :]

    for p in (3, 4):
        serve_first(p, 2)
        for da in (0, 1, 3, 2)[len(EARLY) :]:
            send_second(p, da)
    yfinish(oblock, oss, ors)
    for cp in local[7:]:
        cp.wait()
    for i in range(1, 8):
        acopy(0, tp, (tp + i) % 8).wait_recv()

    @pl.when(tp >= 4)
    def _():
        acopy(0, tp, tp).wait_recv()

    sq = jnp.zeros((OWN, 1), F32)
    for j in range(D // NB):
        pj = jnp.dot(AT[...], GO[:, j * NB : (j + 1) * NB], preferred_element_type=F32)
        mj = resid_ref[:, j * NB : (j + 1) * NB].astype(F32) + pj
        MIX[:, j * NB : (j + 1) * NB] = mj
        sq = sq + jnp.sum(mj * mj, axis=1, keepdims=True)
    inv = lax.rsqrt(sq * (1.0 / D) + 1e-6)
    own_slot = slot_of(y, c)
    NA[pl.ds(pl.multiple_of(own_slot * OWN, OWN), OWN), :] = (MIX[...] * inv * gain_ref[...]).astype(BF)
    for h in range(2):
        ybegin(*nblock(h))
    relay(3)
    if MIXED:
        serve_first(5, 2)
        for da in (0, 1, 3, 2):
            send_second(5, da)
    relay(4)
    for p in (6,) if MIXED else (5, 6):
        serve_first(p, 2)
        for da in (0, 1, 3, 2):
            send_second(p, da)
    for n in range(2):
        for h in range(2):
            yserve(*nblock(h), n)
    for h in range(2):
        yserve(*nblock(h), 2)
    collect(3)
    collect(4)
    for h in range(2):
        yfinish(*nblock(h))

    def gu(j, _):
        @pl.when(j == R5)
        def _():
            relay(5)

        @pl.when(j == R6)
        def _():
            relay(6)

        gate_up(pl.multiple_of(j * 128, 128), 128)
        return 0

    def gate_up(c0, n):
        rows = pl.ds(c0, n)
        r = lax.dot_general(
            NA[...], jnp.concatenate([GT[rows, :], UT[rows, :]], axis=0), NT, preferred_element_type=F32
        )
        gt = r[:, :n]
        HID[:, rows] = (gt / (1.0 + jnp.exp(-gt)) * r[:, n:]).astype(BF)

    lax.fori_loop(0, 5, gu, 0)
    gate_up(640, 48)
    collect(5)
    collect(6)

    half = 4 * OWN

    def scopy(j):
        view = (slice(None), pl.ds(j * NB, NB))
        return pltpu.make_async_remote_copy(
            src_ref=SB.at[view], dst_ref=RB.at[view], send_sem=bss.at[j], recv_sem=brs.at[j],
            device_id=(sp, sib), device_id_type=MESH,
        )

    def rcopy(n, j, to):
        view = (n, slice(None), pl.ds(j * NB, NB))
        return pltpu.make_async_remote_copy(
            src_ref=TB.at[view], dst_ref=RR.at[view], send_sem=css.at[n, j], recv_sem=crs.at[n, j],
            device_id=(sp, tpof(yat(to), c)), device_id_type=MESH,
        )

    def ocopy(j):
        view = (slice(None), pl.ds(j * NB, NB))
        return pltpu.make_async_copy(out_ref.at[view], out_hbm.at[view], osem.at[j])

    def both(n, j):
        view = (pl.ds(pl.multiple_of(yat(n) * OWN, OWN), OWN), slice(j * NB, (j + 1) * NB))
        return PA[view] + RB[view].astype(F32)

    hs = HID[pl.ds(pl.multiple_of((1 - c) * half, half), half), :]
    ho = HID[pl.ds(pl.multiple_of(c * half, half), half), :]
    def pass_on(j):
        cols = slice(j * NB, (j + 1) * NB)
        scopy(j).wait_recv()
        TB[0, :, cols] = both(2, j).astype(BF)
        rcopy(0, j, dy).start()
        TB[1, :, cols] = both(-dy, j).astype(BF)
        rcopy(1, j, -dy).start()

    for j in range(NC):
        cols = slice(j * NB, (j + 1) * NB)
        SB[:, cols] = jnp.dot(hs, GD[:, cols], preferred_element_type=F32).astype(BF)
        scopy(j).start()
        PA[:, cols] = jnp.dot(ho, GD[:, cols], preferred_element_type=F32)
        if j > 0:
            pass_on(j - 1)
    pass_on(NC - 1)
    for p in range(N_PIECE):

        def drain(i, _):
            copy(p, sp, i, sp).wait_send()
            return 0

        lax.fori_loop(0, 15, drain, 0)
    for i in range(7):
        ycopy(oblock, oss, ors, i, slot_of(y, c), sib).wait_send()
        for h in range(2):
            ycopy(*nblock(h), i, slot_of(y, c), sib).wait_send()
    for i in range(1, 8):
        acopy(i, tp, tp).wait_send()

    @pl.when(tp >= 4)
    def _():
        acopy(0, tp, tp).wait_send()

    qcopy().wait_send()
    for j in range(NC):
        cols = slice(j * NB, (j + 1) * NB)
        rcopy(0, j, dy).wait_recv()
        TB[2, :, cols] = (both(dy, j) + RR[0, :, cols].astype(F32)).astype(BF)
        rcopy(2, j, dy).start()
    for j in range(NC):
        cols = slice(j * NB, (j + 1) * NB)
        rcopy(1, j, -dy).wait_recv()
        rcopy(2, j, dy).wait_recv()
        ffn = both(0, j) + RR[1, :, cols].astype(F32) + RR[2, :, cols].astype(F32)
        out_ref[:, cols] = (MIX[:, cols] + 0.5 * ffn).astype(BF)
        ocopy(j).start()

    for j in range(NC):
        for n in range(3):
            rcopy(n, j, dy).wait_send()
        scopy(j).wait_send()
    for j in range(NC):
        ocopy(j).wait()


def local(resid, queries, keys, values, cum_gate, out_weight, norm_gain, gate_weight, up_weight, down_weight):
    hbm = pl.BlockSpec(memory_space=pl.ANY)
    dma = pltpu.SemaphoreType.DMA
    V = pltpu.VMEM
    return pl.pallas_call(
        kernel,
        out_shape=jax.ShapeDtypeStruct((OWN, D), BF),
        in_specs=[hbm] * 10,
        out_specs=hbm,
        scratch_shapes=[
            V((N_SP, 2, ROWS), F32),
            V((N_SP * ROWS, 128), BF),
            V((N_SP * ROWS, 128), BF),
            V((FFW, D), BF),
            V((FFW, D), BF),
            V((FFW, D), BF),
            V((1024, D), BF),
            V((HQ, 128), BF),
            V((2, ROWS, 128), BF),
            V((2, ROWS, 256), F32),
            V((2, ROWS, 128), F32),
            V((ROWS, 128), BF),
            V((OWN, 1024), BF),
            V((OWN, D), F32),
            V((ROWS, D), BF),
            V((ROWS, FFW), BF),
            V((4 * OWN, D), BF),
            V((4 * OWN, D), BF),
            V((4 * OWN, D), F32),
            V((3, OWN, D), BF),
            V((3, OWN, D), BF),
            V((ROWS, 128), BF),
            V((OWN, D), BF),
            V((1, D), F32),
            V((OWN, D), BF),
            dma((N_PIECE, N_SP)),
            dma((N_PIECE, 15)),
            dma((8,)),
            dma((7,)),
            dma((2, 8)),
            dma((2, 7)),
            dma((8,)),
            dma((8,)),
            dma((NC,)),
            dma((NC,)),
            dma((3, NC)),
            dma((3, NC)),
            dma((10,)),
            dma((2,)),
            dma((NC,)),
        ],
        compiler_params=pltpu.CompilerParams(
            collective_id=0, has_side_effects=True, vmem_limit_bytes=64 * 1024 * 1024 - 128 * 1024
        ),
        name="layer",
    )(
        queries, keys, values, cum_gate.T, out_weight, gate_weight.T, up_weight.T, down_weight, resid,
        norm_gain.reshape(1, D),
    )


def solution(mesh):
    return jax.shard_map(
        local,
        mesh=mesh,
        in_specs=(
            P(("sp", "tp"), None),
            P("sp", "tp"),
            P("sp", "tp"),
            P("sp", "tp"),
            P("sp", "tp"),
            P("tp", None),
            P(),
            P("sp", "tp"),
            P("sp", "tp"),
            P("tp", "sp"),
        ),
        out_specs=P(("sp", "tp"), None),
        check_vma=False,
    )
```

```python
import functools

import jax
import jax.numpy as jnp
from jax import lax
from jax.experimental import pallas as pl
from jax.experimental.pallas import tpu as pltpu
from jax.sharding import PartitionSpec as P

HEAD_DIM = 64
ROWS = 768
OWN = 96
D = 2048
FFW = 688
N_SP = 16
NB = 256
NC = D // NB
HQ = ROWS // 2
QROWS = 384
AHEAD = 1
R5 = 0
R6 = 2
KV = (1, 2, 0)
LOOK = 0
EARLY = (0,)
MIXED = False
K_O1 = 6
K_O2 = 10
K_W = 8
K_WS = 13
WEIGHTS = (3, 4, 5, 6)
BF = jnp.bfloat16
F32 = jnp.float32
MESH = pl.DeviceIdType.MESH
NT = (((1,), (1,)), ((), ()))

N_PIECE = 7
SIGN = (1, 1, -1, 1, -1, 1, -1)


WAVE = (
    (0, 0), (1, 0), (3, 0), (0, 1), (0, 3), (2, 0), (1, 1), (3, 1),
    (1, 3), (3, 3), (0, 2), (2, 1), (2, 3), (1, 2), (3, 2), (2, 2),
)


def offsets(k):
    if isinstance(k, int):
        return WAVE[k]
    da, db = jnp.int32(0), jnp.int32(0)
    for n in range(1, 16):
        da = jnp.where(k == n, WAVE[n][0], da)
        db = jnp.where(k == n, WAVE[n][1], db)
    return da, db


def kernel(
    q_in, k_ref, v_ref, g_ref, ow_ref, wg_ref, wu_ref, wd_ref, resid_in, gain_in,
    out_hbm,
    GG, GK, GV, GT, UT, GD, GO, QR, QZ, ACC, MX, ATL, AT, MIX, NA, HID, SB, RB, PA, TB, RR,
    q_ref, resid_ref, gain_ref, out_ref,
    rs, ss, ors, oss, nrs, nss, ars, ass, brs, bss, crs, css, lsem, qsem, osem,
):
    sp = lax.axis_index("sp")
    tp = lax.axis_index("tp")
    c = tp % 2
    y = tp // 2
    z = sp // 4
    x = sp % 4
    a = z + c * (x - z)
    b = x + c * (z - x)

    def spof(da, db):
        return ((a + da + 4) % 4) * (4 - 3 * c) + ((b + db + 4) % 4) * (1 + 3 * c)

    def tpof(yy, cc):
        return yy * 2 + cc

    sib = tpof(y, 1 - c)
    ps = N_SP - 1 - sp

    bar = pltpu.get_barrier_semaphore()
    for da, db in ((1, 0), (3, 0), (0, 1), (0, 3)):
        pl.semaphore_signal(bar, inc=1, device_id=(spof(da, db), tp), device_id_type=MESH)
    for i in range(8):
        if i:
            pl.semaphore_signal(bar, inc=1, device_id=(sp, (tp + i) % 8), device_id_type=MESH)
        pl.semaphore_signal(bar, inc=1, device_id=(ps, (tp + i) % 8), device_id_type=MESH)

    def part(p, s):
        if p == 0:
            return GG.at[s]
        if p == 1:
            return GK.at[pl.ds(pl.multiple_of(s * ROWS, ROWS), ROWS)]
        if p == 2:
            return GV.at[pl.ds(pl.multiple_of(s * ROWS, ROWS), ROWS)]
        if p == 3:
            return GT.at[:, pl.ds(pl.multiple_of(s * 128, 128), 128)]
        if p == 4:
            return UT.at[:, pl.ds(pl.multiple_of(s * 128, 128), 128)]
        if p == 5:
            return GD.at[pl.ds(0, 352), pl.ds(pl.multiple_of(s * 128, 128), 128)]
        return GD.at[pl.ds(352, 336), pl.ds(pl.multiple_of(s * 128, 128), 128)]

    local = [
        pltpu.make_async_copy(g_ref, part(0, sp), lsem.at[0]),
        pltpu.make_async_copy(k_ref, part(1, sp), lsem.at[1]),
        pltpu.make_async_copy(v_ref, part(2, sp), lsem.at[2]),
        pltpu.make_async_copy(wd_ref, GD.at[:, pl.ds(pl.multiple_of(sp * 128, 128), 128)], lsem.at[3]),
        pltpu.make_async_copy(ow_ref, GO.at[pl.ds(pl.multiple_of(tp * 128, 128), 128)], lsem.at[4]),
        pltpu.make_async_copy(wg_ref, part(3, sp), lsem.at[5]),
        pltpu.make_async_copy(wu_ref, part(4, sp), lsem.at[6]),
        pltpu.make_async_copy(resid_in, resid_ref, lsem.at[7]),
        pltpu.make_async_copy(gain_in, gain_ref, lsem.at[8]),
    ]
    q_local = pltpu.make_async_copy(q_in, q_ref, lsem.at[9])
    for cp in [q_local] + local:
        cp.start()

    def copy(p, s, idx, dst):
        return pltpu.make_async_remote_copy(
            src_ref=part(p, s), dst_ref=part(p, s), send_sem=ss.at[p, idx], recv_sem=rs.at[p, s],
            device_id=(dst, tp), device_id_type=MESH,
        )

    def begin_first(p):
        copy(p, sp, 0, spof(1, 0)).start()
        copy(p, sp, 1, spof(3, 0)).start()

    def send_second(p, da):
        s = spof(da, 0)
        copy(p, s, 2 + 2 * da, spof(0, 1)).start()
        copy(p, s, 3 + 2 * da, spof(0, 3)).start()

    def begin(p):
        begin_first(p)
        send_second(p, 0)

    def serve_first(p, da):
        s = spof(da, 0)
        copy(p, s, 0, sp).wait_recv()
        d = SIGN[p]
        if da == (4 - d) % 4:
            copy(p, s, 10, spof(d, 0)).start()

    def onward(p, da):
        return SIGN[p] * (1 - 2 * (da % 2))

    def relay(p):
        for da in (0, 1, 3, 2):
            d = onward(p, da)
            s = spof(da, 4 - d)
            copy(p, s, 0, sp).wait_recv()
            copy(p, s, 11 + da, spof(0, d)).start()

    def collect(p):
        for da in (0, 1, 3, 2):
            for db in (4 + onward(p, da), 2):
                copy(p, spof(da, db), 0, sp).wait_recv()

    def serve(p, k):
        da, db = offsets(k)
        s = spof(da, db)
        copy(p, s, 0, sp).wait_recv()
        d = SIGN[p]
        back = (4 - d) % 4

        @pl.when((db == 0) & (da == back))
        def _():
            copy(p, s, 10, spof(d, 0)).start()

        @pl.when(db == 0)
        def _():
            copy(p, s, 2 + 2 * da, spof(0, 1)).start()
            copy(p, s, 3 + 2 * da, spof(0, 3)).start()

        @pl.when(db == back)
        def _():
            copy(p, s, 11 + da, spof(0, d)).start()

    dy = 1 - 2 * c

    def yat(n):
        return (y + n + 4) % 4

    def ycopy(block, sems, rsems, idx, slot, dst):
        return pltpu.make_async_remote_copy(
            src_ref=block(slot), dst_ref=block(slot), send_sem=sems.at[idx], recv_sem=rsems.at[slot],
            device_id=(sp, dst), device_id_type=MESH,
        )

    def slot_of(yy, cc):
        return cc * 4 + yy

    def ybegin(block, sems, rsems):
        own = slot_of(y, c)
        ycopy(block, sems, rsems, 0, own, tpof(yat(dy), c)).start()
        ycopy(block, sems, rsems, 1, own, tpof(yat(-dy), c)).start()
        ycopy(block, sems, rsems, 2, own, sib).start()

    def yserve(block, sems, rsems, n):
        if n == 0:
            s = slot_of(yat(-dy), c)
            ycopy(block, sems, rsems, 0, s, sib).wait_recv()
            ycopy(block, sems, rsems, 3, s, tpof(yat(dy), c)).start()
            ycopy(block, sems, rsems, 4, s, sib).start()
        elif n == 1:
            s = slot_of(yat(dy), c)
            ycopy(block, sems, rsems, 0, s, sib).wait_recv()
            ycopy(block, sems, rsems, 5, s, sib).start()
        else:
            s = slot_of(yat(2), c)
            ycopy(block, sems, rsems, 0, s, sib).wait_recv()
            ycopy(block, sems, rsems, 6, s, sib).start()

    def yfinish(block, sems, rsems):
        for n in range(4):
            s = slot_of(yat(n), 1 - c)
            ycopy(block, sems, rsems, 0, s, sib).wait_recv()

    def oblock(slot):
        t = (slot % 4) * 2 + slot // 4
        return GO.at[pl.ds(pl.multiple_of(t * 128, 128), 128)]

    def nblock(part):
        def view(slot):
            return NA.at[pl.ds(pl.multiple_of(slot * OWN, OWN), OWN), pl.ds(part * (D // 2), D // 2)]

        return view, nss.at[part], nrs.at[part]

    half_lane = lax.broadcasted_iota(jnp.int32, (HQ, 128), 1)

    def spread(half, q):
        qs = q.astype(F32) * (HEAD_DIM ** (-0.5))
        QZ[half, :HQ, :] = jnp.where(half_lane < HEAD_DIM, qs, 0.0).astype(BF)
        QZ[half, HQ:, :] = jnp.where(half_lane >= HEAD_DIM, qs, 0.0).astype(BF)

    def qcopy():
        return pltpu.make_async_remote_copy(
            src_ref=q_ref.at[pl.ds(HQ, HQ)], dst_ref=QR, send_sem=qsem.at[0], recv_sem=qsem.at[1],
            device_id=(ps, tp), device_id_type=MESH,
        )

    for cp in [q_local] + local[:3]:
        cp.wait()
    pl.semaphore_wait(bar, 19)
    qcopy().start()
    for p in KV:
        begin_first(p)
        send_second(p, 0)
    local[4].wait()
    ybegin(oblock, oss, ors)
    spread(0, q_ref[:HQ, :])
    ACC[1] = jnp.zeros((2 * HQ, 256), F32)
    MX[1] = jnp.full((2 * HQ, 128), -1e30, F32)

    def values_of(s, width):
        vb = GV[pl.ds(pl.multiple_of(s * ROWS, ROWS), width), :]
        return jnp.concatenate([vb, jnp.ones((width, 128), BF)], axis=1)

    def attend(half, s, width, first_key, is_first):
        kb = GK[pl.ds(pl.multiple_of(s * ROWS, ROWS), width), :]
        vb = values_of(s, width)
        count = 2 * HQ // QROWS

        def score(n):
            return lax.dot_general(
                QZ[half, n * QROWS : (n + 1) * QROWS, :], kb, NT, preferred_element_type=F32
            )

        def finish(n, sc):
            h, r0 = divmod(n * QROWS, HQ)
            rows = slice(n * QROWS, (n + 1) * QROWS)
            sh = sc - GG[s, h : h + 1, :width]
            if first_key is not None:
                row = lax.broadcasted_iota(jnp.int32, (QROWS, width), 0) + (first_key + r0)
                col = lax.broadcasted_iota(jnp.int32, (QROWS, width), 1)
                sh = jnp.where(col <= row, sh, -1e30)
            top = jnp.max(sh, axis=1, keepdims=True)
            if is_first:
                top = jnp.broadcast_to(top, (QROWS, 128))
            else:
                old = MX[half, rows, :]
                top = jnp.maximum(old, top)
            wt = jnp.exp(sh - jnp.concatenate([top] * (width // 128), axis=1)).astype(BF)
            pv = jnp.dot(wt, vb, preferred_element_type=F32)
            if is_first:
                ACC[half, rows, :] = pv
            else:
                fade = jnp.exp(old - top)
                ACC[half, rows, :] = ACC[half, rows, :] * jnp.concatenate([fade, fade], axis=1) + pv
            MX[half, rows, :] = top

        held = [score(n) for n in range(AHEAD)]
        for n in range(count):
            if n + AHEAD < count:
                held.append(score(n + AHEAD))
            finish(n, held[n])

    attend(0, sp, HQ, 0, True)
    qcopy().wait_recv()
    spread(1, QR[...])
    for cp in local[5:7]:
        cp.wait()
    local[3].wait()
    for k in range(1, LOOK):
        for p in KV:
            serve(p, k)

    def step(k, _):
        @pl.when((k + LOOK < N_SP) & (k + LOOK > 0))
        def _():
            for p in KV:
                serve(p, k + LOOK)

        @pl.when(k == K_O1)
        def _():
            yserve(oblock, oss, ors, 0)
            yserve(oblock, oss, ors, 1)

        @pl.when(k == K_O2)
        def _():
            yserve(oblock, oss, ors, 2)

        @pl.when(k == K_W)
        def _():
            for p in WEIGHTS:
                begin_first(p)

        @pl.when(k == K_WS)
        def _():
            for p in WEIGHTS:
                serve_first(p, 1)
                serve_first(p, 3)
                if p < 5:
                    for da in EARLY:
                        send_second(p, da)

        s = spof(*offsets(k))

        @pl.when(s < sp)
        def _():
            attend(0, s, ROWS, None, False)

        @pl.when(s < ps)
        def _():
            attend(1, s, ROWS, None, False)

        @pl.when(s == ps)
        def _():
            attend(1, s, ROWS, HQ, False)

        return 0

    lax.fori_loop(0, N_SP, step, 0)

    for half in range(2):
        o0 = ACC[half, :HQ, :128] / ACC[half, :HQ, 128:]
        o1 = ACC[half, HQ:, :128] / ACC[half, HQ:, 128:]
        ATL[half * HQ : (half + 1) * HQ, :] = jnp.where(half_lane < HEAD_DIM, o0, o1).astype(BF)

    def acopy(i, dst, slot):
        return pltpu.make_async_remote_copy(
            src_ref=ATL.at[pl.ds(pl.multiple_of(dst * OWN, 32), OWN)],
            dst_ref=AT.at[:, pl.ds(pl.multiple_of(slot * 128, 128), 128)],
            send_sem=ass.at[i], recv_sem=ars.at[slot],
            device_id=(sp + (dst // 4) * (ps - sp), dst), device_id_type=MESH,
        )

    for i in range(1, 8):
        acopy(i, (tp + i) % 8, tp).start()

    @pl.when(tp >= 4)
    def _():
        acopy(0, tp, tp).start()

    @pl.when(tp < 4)
    def _():
        AT[:, pl.ds(pl.multiple_of(tp * 128, 128), 128)] = ATL[pl.ds(pl.multiple_of(tp * OWN, 32), OWN), :]

    for p in (3, 4):
        serve_first(p, 2)
        for da in (0, 1, 3, 2)[len(EARLY) :]:
            send_second(p, da)
    yfinish(oblock, oss, ors)
    for cp in local[7:]:
        cp.wait()
    for i in range(1, 8):
        acopy(0, tp, (tp + i) % 8).wait_recv()

    @pl.when(tp >= 4)
    def _():
        acopy(0, tp, tp).wait_recv()

    sq = jnp.zeros((OWN, 1), F32)
    for j in range(D // NB):
        pj = jnp.dot(AT[...], GO[:, j * NB : (j + 1) * NB], preferred_element_type=F32)
        mj = resid_ref[:, j * NB : (j + 1) * NB].astype(F32) + pj
        MIX[:, j * NB : (j + 1) * NB] = mj
        sq = sq + jnp.sum(mj * mj, axis=1, keepdims=True)
    inv = lax.rsqrt(sq * (1.0 / D) + 1e-6)
    own_slot = slot_of(y, c)
    NA[pl.ds(pl.multiple_of(own_slot * OWN, OWN), OWN), :] = (MIX[...] * inv * gain_ref[...]).astype(BF)
    for h in range(2):
        ybegin(*nblock(h))
    relay(3)
    if MIXED:
        serve_first(5, 2)
        for da in (0, 1, 3, 2):
            send_second(5, da)
    relay(4)
    for p in (6,) if MIXED else (5, 6):
        serve_first(p, 2)
        for da in (0, 1, 3, 2):
            send_second(p, da)
    for n in range(2):
        for h in range(2):
            yserve(*nblock(h), n)
    for h in range(2):
        yserve(*nblock(h), 2)
    collect(3)
    collect(4)
    for h in range(2):
        yfinish(*nblock(h))

    def gu(j, _):
        @pl.when(j == R5)
        def _():
            relay(5)

        @pl.when(j == R6)
        def _():
            relay(6)

        gate_up(pl.multiple_of(j * 128, 128), 128)
        return 0

    def gate_up(c0, n):
        rows = pl.ds(c0, n)
        r = lax.dot_general(
            NA[...], jnp.concatenate([GT[rows, :], UT[rows, :]], axis=0), NT, preferred_element_type=F32
        )
        gt = r[:, :n]
        HID[:, rows] = (gt / (1.0 + jnp.exp(-gt)) * r[:, n:]).astype(BF)

    lax.fori_loop(0, 5, gu, 0)
    gate_up(640, 48)
    collect(5)
    collect(6)

    half = 4 * OWN

    def scopy(j):
        view = (slice(None), pl.ds(j * NB, NB))
        return pltpu.make_async_remote_copy(
            src_ref=SB.at[view], dst_ref=RB.at[view], send_sem=bss.at[j], recv_sem=brs.at[j],
            device_id=(sp, sib), device_id_type=MESH,
        )

    def rcopy(n, j, to):
        view = (n, slice(None), pl.ds(j * NB, NB))
        return pltpu.make_async_remote_copy(
            src_ref=TB.at[view], dst_ref=RR.at[view], send_sem=css.at[n, j], recv_sem=crs.at[n, j],
            device_id=(sp, tpof(yat(to), c)), device_id_type=MESH,
        )

    def ocopy(j):
        view = (slice(None), pl.ds(j * NB, NB))
        return pltpu.make_async_copy(out_ref.at[view], out_hbm.at[view], osem.at[j])

    def both(n, j):
        view = (pl.ds(pl.multiple_of(yat(n) * OWN, OWN), OWN), slice(j * NB, (j + 1) * NB))
        return PA[view] + RB[view].astype(F32)

    hs = HID[pl.ds(pl.multiple_of((1 - c) * half, half), half), :]
    ho = HID[pl.ds(pl.multiple_of(c * half, half), half), :]
    def pass_on(j):
        cols = slice(j * NB, (j + 1) * NB)
        scopy(j).wait_recv()
        TB[0, :, cols] = both(2, j).astype(BF)
        rcopy(0, j, dy).start()
        TB[1, :, cols] = both(-dy, j).astype(BF)
        rcopy(1, j, -dy).start()

    for j in range(NC):
        cols = slice(j * NB, (j + 1) * NB)
        SB[:, cols] = jnp.dot(hs, GD[:, cols], preferred_element_type=F32).astype(BF)
        scopy(j).start()
        PA[:, cols] = jnp.dot(ho, GD[:, cols], preferred_element_type=F32)
        if j > 0:
            pass_on(j - 1)
    pass_on(NC - 1)
    for p in range(N_PIECE):

        def drain(i, _):
            copy(p, sp, i, sp).wait_send()
            return 0

        lax.fori_loop(0, 15, drain, 0)
    for i in range(7):
        ycopy(oblock, oss, ors, i, slot_of(y, c), sib).wait_send()
        for h in range(2):
            ycopy(*nblock(h), i, slot_of(y, c), sib).wait_send()
    for i in range(1, 8):
        acopy(i, tp, tp).wait_send()

    @pl.when(tp >= 4)
    def _():
        acopy(0, tp, tp).wait_send()

    qcopy().wait_send()
    for j in range(NC):
        cols = slice(j * NB, (j + 1) * NB)
        rcopy(0, j, dy).wait_recv()
        TB[2, :, cols] = (both(dy, j) + RR[0, :, cols].astype(F32)).astype(BF)
        rcopy(2, j, dy).start()
    for j in range(NC):
        scopy(j).wait_send()
        for n in range(2):
            rcopy(n, j, dy).wait_send()
    for j in range(NC):
        cols = slice(j * NB, (j + 1) * NB)
        rcopy(1, j, -dy).wait_recv()
        rcopy(2, j, dy).wait_recv()
        ffn = both(0, j) + RR[1, :, cols].astype(F32) + RR[2, :, cols].astype(F32)
        out_ref[:, cols] = (MIX[:, cols] + 0.5 * ffn).astype(BF)
        ocopy(j).start()

    for j in range(NC):
        rcopy(2, j, dy).wait_send()
    for j in range(NC):
        ocopy(j).wait()


def local(resid, queries, keys, values, cum_gate, out_weight, norm_gain, gate_weight, up_weight, down_weight):
    hbm = pl.BlockSpec(memory_space=pl.ANY)
    dma = pltpu.SemaphoreType.DMA
    V = pltpu.VMEM
    return pl.pallas_call(
        kernel,
        out_shape=jax.ShapeDtypeStruct((OWN, D), BF),
        in_specs=[hbm] * 10,
        out_specs=hbm,
        scratch_shapes=[
            V((N_SP, 2, ROWS), F32),
            V((N_SP * ROWS, 128), BF),
            V((N_SP * ROWS, 128), BF),
            V((FFW, D), BF),
            V((FFW, D), BF),
            V((FFW, D), BF),
            V((1024, D), BF),
            V((HQ, 128), BF),
            V((2, ROWS, 128), BF),
            V((2, ROWS, 256), F32),
            V((2, ROWS, 128), F32),
            V((ROWS, 128), BF),
            V((OWN, 1024), BF),
            V((OWN, D), F32),
            V((ROWS, D), BF),
            V((ROWS, FFW), BF),
            V((4 * OWN, D), BF),
            V((4 * OWN, D), BF),
            V((4 * OWN, D), F32),
            V((3, OWN, D), BF),
            V((3, OWN, D), BF),
            V((ROWS, 128), BF),
            V((OWN, D), BF),
            V((1, D), F32),
            V((OWN, D), BF),
            dma((N_PIECE, N_SP)),
            dma((N_PIECE, 15)),
            dma((8,)),
            dma((7,)),
            dma((2, 8)),
            dma((2, 7)),
            dma((8,)),
            dma((8,)),
            dma((NC,)),
            dma((NC,)),
            dma((3, NC)),
            dma((3, NC)),
            dma((10,)),
            dma((2,)),
            dma((NC,)),
        ],
        compiler_params=pltpu.CompilerParams(
            collective_id=0, has_side_effects=True, vmem_limit_bytes=64 * 1024 * 1024 - 128 * 1024
        ),
        name="layer",
    )(
        queries, keys, values, cum_gate.T, out_weight, gate_weight.T, up_weight.T, down_weight, resid,
        norm_gain.reshape(1, D),
    )


def solution(mesh):
    return jax.shard_map(
        local,
        mesh=mesh,
        in_specs=(
            P(("sp", "tp"), None),
            P("sp", "tp"),
            P("sp", "tp"),
            P("sp", "tp"),
            P("sp", "tp"),
            P("tp", None),
            P(),
            P("sp", "tp"),
            P("sp", "tp"),
            P("tp", "sp"),
        ),
        out_specs=P(("sp", "tp"), None),
        check_vma=False,
    )
```
